32 devices in a mesh: ep: 8 (over z, core), tp: 4 (over y, x).
Axes of the slice: x: 2, y: 2, z: 4, core: 2. Of those that a mesh axis runs over, the one named last changes fastest.
Arguments:
- query_rows: bfloat16 [6144, 1024], P('ep', 'tp'), may hold values from -600 to 600
- key_rows: bfloat16 [6144, 1024], P('ep', 'tp'), may hold values from -6 to 6
- value_rows: bfloat16 [6144, 1024], P('ep', 'tp'), may hold values from -6 to 6
- cum_gate: float32 [16, 6144], P('tp'), may hold values from -615 to 0, as said below
- out_weight: bfloat16 [1024, 2048], P(None, 'tp'), may hold values from -0.1875 to 0.1875
- moe_input: bfloat16 [1536, 2048], P('ep'), may hold values from -6 to 6
- moe_gain: float32 [2048], replicated, may hold values from 0.1 to 1.9
- routes: int32 [1536, 3], P('ep'), may hold values from 0 to 31, all different within a row; in each aligned block of 192 rows (0 to 191, 192 to 383, ...) at most 36 rows name the same one
- route_weight: float32 [1536, 3], P('ep'), may hold values from 0.2 to 1.5
- expert_gate: bfloat16 [32, 2048, 512], P('ep', None, 'tp'), may hold values from -0.125 to 0.125
- expert_up: bfloat16 [32, 2048, 512], P('ep', None, 'tp'), may hold values from -0.125 to 0.125
- expert_down: bfloat16 [32, 512, 2048], P('ep', None, 'tp'), may hold values from -0.25 to 0.25
- shared_gate: bfloat16 [2048, 512], P(None, 'tp'), may hold values from -0.125 to 0.125
- shared_up: bfloat16 [2048, 512], P(None, 'tp'), may hold values from -0.125 to 0.125
- shared_down: bfloat16 [512, 2048], P(None, 'tp'), may hold values from -0.25 to 0.25
Outputs:
- mixer_out: bfloat16 [6144, 2048], P('ep', 'tp')
- moe_out: bfloat16 [1536, 2048], P('ep', 'tp')
The draws below stay inside these ranges and needn't reach their ends.
Inputs may be any that keep to these rules, and one draw needn't show every extreme that they name: Non-increasing along positions: cum_gate[h, t] is the sum of the log forget gates of head h over positions 0 to t. `routes`: the 3 experts of a token differ. In each aligned block of 192 tokens no expert is named by more than 36 tokens, a bound that some block reaches.
All inputs are finite; a program needn't handle non-finite values.
Results may differ from the reference program's by a relative error of at most 0.0068.
Values may be sent and summed in bfloat16 or wider, within the bound.
A program may use at most 64 MiB of HBM per device.

```python
import math
import jax
import jax.numpy as jnp
import numpy as np
from jax import lax

D = 2048
HEADS = 16
HEAD = 64
FF = 512
FS = 512
EXPERTS = 32
TOP = 3
SEQ_DEV = 768
LENGTH = 6144
MOE_DEV = 192
TOKENS_MOE = 1536
CAP = 36
N_EP = 8


def draw_query_rows(key, part):
    base_key = jax.random.fold_in(key, 7)
    key_normal = jax.random.fold_in(base_key, 0)
    drawn = jnp.clip(jax.random.normal(key_normal, (LENGTH, HEADS * HEAD), jnp.float32), -6.0, 6.0)
    return drawn.astype(jnp.bfloat16)


def draw_cum_gate(key, part):
    base_key = jax.random.fold_in(key, 13)
    key_heads, key_steps, key_blocks = jax.random.split(base_key, 3)
    head_order = jax.random.permutation(key_heads, HEADS)
    fast_count = HEADS // 2
    decay_rates = jnp.where(head_order < fast_count, 1.0 / 40.0, 1.0 / LENGTH).astype(jnp.float32)
    low = jnp.log(0.5)
    high = jnp.log(2.0)
    step_factors = jnp.exp(jax.random.uniform(key_steps, (HEADS, LENGTH), jnp.float32, low, high))
    block_factors = jnp.exp(jax.random.uniform(key_blocks, (HEADS, LENGTH // SEQ_DEV), jnp.float32, low, high))
    block_factors = jnp.repeat(block_factors, SEQ_DEV, axis=1)
    log_gates = -decay_rates[:, None] * step_factors * block_factors
    return jnp.cumsum(log_gates, axis=1).astype(jnp.float32)


def levels(rng, shape, cuts, least, high):
    def one(axis_at, shards_of):
        draws = jax.random.uniform(jax.random.fold_in(jax.random.fold_in(rng, 6), axis_at), (shards_of,), jnp.float32, least / len(cuts), high / len(cuts))
        return jnp.repeat(jnp.exp(draws), shape[axis_at] // shards_of).reshape((-1,) + (1,) * (len(shape) - axis_at - 1))

    loudness = one(*cuts[0])
    for cut in cuts[1:]:
        loudness = loudness * one(*cut)
    return loudness


def deal_out(rng, own, number, rows, amount, top, limit, slope):
    order = jax.random.permutation(rng, amount)
    heavy_load, common = load_shares(amount, rows * top, limit, slope, True), load_shares(amount, rows * top, limit, slope, False)
    places = jnp.arange(amount)

    def named(tallies, turn):
        used = int((tallies > 0).sum())
        fixed = max(1, used // 4)
        shifted = fixed + (places - fixed + turn * (used - fixed)) % max(1, amount - fixed)
        return jnp.zeros((amount,), jnp.int32).at[order[jnp.where(places < fixed, places, shifted)]].set(jnp.asarray(tallies, jnp.int32))

    tallies = jnp.where(number % 4 == 0, named(heavy_load, number // 4), named(common, number - number // 4 - 1))
    mixed = jax.random.permutation(jax.random.fold_in(own, 3), amount)
    donor, receiver = mixed[0:amount // 2 * 2:2], mixed[1:amount // 2 * 2:2]
    margin = jnp.minimum(tallies[donor] - 1, limit - tallies[receiver]) // 2
    margin = jnp.where((donor == order[0]) | (receiver == order[0]) | (tallies[receiver] == 0), 0, jnp.maximum(margin, 0))
    shifted = jax.random.randint(jax.random.fold_in(own, 4), (amount // 2,), 0, 1 << 20) % (margin + 1)
    tallies = tallies.at[donor].add(-shifted).at[receiver].add(shifted)
    members = jnp.searchsorted(jnp.cumsum(tallies), jnp.arange(rows * top), side="right").astype(jnp.int32)
    listing = members.reshape(top, rows).T
    listing = listing[jax.random.permutation(jax.random.fold_in(own, 1), rows)]
    turn = jax.random.randint(jax.random.fold_in(own, 2), (rows, 1), 0, top)
    return jnp.take_along_axis(listing, (jnp.arange(top)[None, :] + turn) % top, axis=1)


def load_shares(amount, total, reach, skew, full):
    portions = [(1 << 20) // math.isqrt(standing ** skew) + 1 for standing in range(1, amount + 1)]
    largest = reach if full else min(reach, max(-(-total // amount), total * portions[0] // sum(portions)))
    least = 1 if total - largest >= amount - 1 else 0
    holding, rest = [largest] + [least] * (amount - 1), total - largest - least * (amount - 1)
    while rest > 0:
        free = [i for i in range(1, amount) if holding[i] < largest] or [i for i in range(1, amount) if holding[i] < reach]
        pool, left = sum([portions[i] for i in free]), rest
        for i in free:
            more = min(reach - holding[i], max(1, left * portions[i] // pool), rest)
            holding[i] = holding[i] + more
            rest = rest - more
    return np.array(holding)


def bell_draw(stream_key, shape, deviation, limit, cuts=(), kind=jnp.bfloat16):
    array = jax.random.normal(stream_key, shape, jnp.float32) * deviation
    if len(cuts) > 0:
        array = levels(stream_key, shape, cuts, -0.22, 0.18) * array
    return jnp.clip(array, min=-limit, max=limit).astype(kind)


def setup_inputs(seed: int = 0) -> dict:
    keys = jax.random.split(jax.random.key(seed), 16)
    query_rows = draw_query_rows(jax.random.fold_in(keys[15], 71), 0)
    key_rows = bell_draw(keys[1], (LENGTH, HEADS * HEAD), 1.0, 6.0, ((0, 8), (1, 4)))
    value_rows = bell_draw(keys[2], (LENGTH, HEADS * HEAD), 1.0, 6.0, ((0, 8), (1, 4)))
    cum_gate = draw_cum_gate(jax.random.fold_in(keys[15], 71), 0)
    out_weight = bell_draw(keys[4], (HEADS * HEAD, D), (HEADS * HEAD) ** -0.5, 0.1875, ((1, 4),))
    moe_input = bell_draw(keys[5], (TOKENS_MOE, D), 1.0, 6.0, ((0, 8),))
    moe_gain = jnp.clip(1.0 + 0.18 * jax.random.normal(keys[6], (D,), jnp.float32), 0.1, 1.9)
    routes_keys = jax.random.split(jax.random.fold_in(keys[7], 1), TOKENS_MOE // MOE_DEV)
    routes_turns = jax.random.permutation(jax.random.fold_in(keys[7], 3), TOKENS_MOE // MOE_DEV)
    routes = jax.vmap(lambda own, number: deal_out(jax.random.fold_in(keys[7], 2), own, number, MOE_DEV, EXPERTS, TOP, CAP, 2))(routes_keys, routes_turns).reshape((TOKENS_MOE, TOP))
    route_weight = jnp.clip(jnp.exp(math.log(1.5) - 2.014903 * jax.random.uniform(keys[8], (TOKENS_MOE, TOP), jnp.float32) ** levels(keys[8], (TOKENS_MOE, TOP), ((0, 8),), -0.2, 0.2)), 0.2, 1.5)
    expert_gate = bell_draw(keys[9], (EXPERTS, D, FF), D ** -0.5, 0.125, ((0, 8), (2, 4)))
    expert_up = bell_draw(keys[10], (EXPERTS, D, FF), D ** -0.5, 0.125, ((0, 8), (2, 4)))
    expert_down = bell_draw(keys[11], (EXPERTS, FF, D), FF ** -0.5, 0.25, ((0, 8), (2, 4)))
    shared_gate = bell_draw(keys[12], (D, FS), D ** -0.5, 0.125, ((1, 4),))
    shared_up = bell_draw(keys[13], (D, FS), D ** -0.5, 0.125, ((1, 4),))
    shared_down = bell_draw(keys[14], (FS, D), FS ** -0.5, 0.25, ((1, 4),))
    return {"query_rows": query_rows, "key_rows": key_rows, "value_rows": value_rows, "cum_gate": cum_gate, "out_weight": out_weight, "moe_input": moe_input, "moe_gain": moe_gain, "routes": routes, "route_weight": route_weight, "expert_gate": expert_gate, "expert_up": expert_up, "expert_down": expert_down, "shared_gate": shared_gate, "shared_up": shared_up, "shared_down": shared_down}


neg_fill = -1e+30
norm_eps = 1e-06

def attention_heads(query_rows, key_rows, value_rows, cum_gate):
    query_span = 128 if LENGTH % 128 == 0 else LENGTH
    query_heads = query_rows.reshape(LENGTH, HEADS, HEAD)
    key_heads = key_rows.reshape(LENGTH, HEADS, HEAD).astype(jnp.float32)
    value_heads = value_rows.reshape(LENGTH, HEADS, HEAD).astype(jnp.float32)
    key_pos = jnp.arange(LENGTH, dtype=jnp.int32)
    scale = HEAD ** (-0.5)

    def one_block(block_index):
        start = (block_index * query_span).astype(jnp.int32)
        query_block = lax.dynamic_slice_in_dim(query_heads, start, query_span, 0).astype(jnp.float32)
        query_gate = lax.dynamic_slice_in_dim(cum_gate, start, query_span, 1)
        scores = jnp.einsum('qhd,khd->hqk', query_block, key_heads) * scale
        scores = scores + query_gate[:, :, None] - cum_gate[:, None, :]
        query_pos = start + jnp.arange(query_span, dtype=jnp.int32)
        causal = key_pos[None, :] <= query_pos[:, None]
        scores = jnp.where(causal[None], scores, neg_fill)
        row_max = lax.optimization_barrier(jnp.max(scores, axis=2, keepdims=True))
        expon = jnp.where(causal[None], jnp.exp(scores - row_max), 0.0)
        denom = lax.optimization_barrier(jnp.sum(expon, axis=2))
        probs = lax.optimization_barrier(expon.astype(jnp.bfloat16)).astype(jnp.float32)
        summed = jnp.einsum('hqk,khd->qhd', probs, value_heads)
        result = summed / jnp.transpose(denom)[:, :, None]
        return result.astype(jnp.bfloat16).reshape(query_span, HEADS * HEAD)
    blocks = lax.map(one_block, jnp.arange(LENGTH // query_span, dtype=jnp.int32))
    return blocks.reshape(LENGTH, HEADS * HEAD)

def experts_branch(moe_input, moe_gain, routes, route_weight, expert_gate, expert_up, expert_down, shared_gate, shared_up, shared_down):
    moe_rows = moe_input.astype(jnp.float32)
    normed = (moe_rows * lax.rsqrt(lax.optimization_barrier(jnp.mean(moe_rows * moe_rows, axis=1, keepdims=True)) + norm_eps) * moe_gain).astype(jnp.bfloat16)
    pair_count = TOKENS_MOE * TOP
    flat_routes = routes.reshape(-1).astype(jnp.int32)
    one_hot = (flat_routes[:, None] == jnp.arange(EXPERTS, dtype=jnp.int32)[None, :]).astype(jnp.int32)
    one_hot = one_hot.reshape(N_EP, MOE_DEV * TOP, EXPERTS)
    ranks = lax.optimization_barrier(jnp.sum(jnp.cumsum(one_hot, axis=1) * one_hot, axis=2)).reshape(-1) - 1
    block_id = jnp.arange(pair_count, dtype=jnp.int32) // (MOE_DEV * TOP)
    slot_index = (flat_routes * (N_EP * CAP) + block_id * CAP + ranks).astype(jnp.int32)
    pair_token = jnp.arange(pair_count, dtype=jnp.int32) // TOP
    slot_token = jnp.full((EXPERTS * N_EP * CAP,), TOKENS_MOE, jnp.int32).at[slot_index].set(pair_token)
    padded = jnp.concatenate([normed, jnp.zeros((1, D), jnp.bfloat16)], axis=0)

    def one_expert(pieces):
        token_index, gate_w, up_w, down_w = pieces
        gathered = padded[token_index]
        gate_val = jnp.dot(gathered, gate_w, preferred_element_type=jnp.float32)
        up_val = jnp.dot(gathered, up_w, preferred_element_type=jnp.float32)
        hidden = (jax.nn.silu(gate_val) * up_val).astype(jnp.bfloat16)
        return jnp.dot(hidden, down_w, preferred_element_type=jnp.float32).astype(jnp.bfloat16)
    results = lax.map(one_expert, (slot_token.reshape(EXPERTS, N_EP * CAP), expert_gate, expert_up, expert_down))
    picked = results.reshape(EXPERTS * N_EP * CAP, D)[slot_index].astype(jnp.float32).reshape(TOKENS_MOE, TOP, D)
    routed = lax.optimization_barrier(jnp.sum(picked * route_weight[:, :, None], axis=1))
    shared_hidden = (jax.nn.silu(jnp.dot(normed, shared_gate, preferred_element_type=jnp.float32)) * jnp.dot(normed, shared_up, preferred_element_type=jnp.float32)).astype(jnp.bfloat16)
    total = routed + jnp.dot(shared_hidden, shared_down, preferred_element_type=jnp.float32)
    return total.astype(jnp.bfloat16)

def reference(query_rows, key_rows, value_rows, cum_gate, out_weight, moe_input, moe_gain, routes, route_weight, expert_gate, expert_up, expert_down, shared_gate, shared_up, shared_down):
    heads_out = attention_heads(query_rows, key_rows, value_rows, cum_gate)
    mixer_out = jnp.dot(heads_out, out_weight, preferred_element_type=jnp.float32).astype(jnp.bfloat16)
    moe_out = experts_branch(moe_input, moe_gain, routes, route_weight, expert_gate, expert_up, expert_down, shared_gate, shared_up, shared_down)
    return (mixer_out, moe_out)
```

```python
import functools

import jax
import jax.numpy as jnp
from jax import lax
from jax.experimental import pallas as pl
from jax.experimental.pallas import tpu as pltpu
from jax.sharding import PartitionSpec as P

HEAD = 64
LANES = 128
CORES = 2

neg_fill = -1e30
norm_eps = 1e-06


def attention_kernel(
    heads,
    q_ref,
    kv_ref,
    gate_ref,
    normed_ref,
    rank_ref,
    out_ref,
    tokens,
    picks,
    held,
    acc,
    row_max,
    scores_even,
    scores_odd,
    tops_even,
    tops_odd,
    up_send,
    side_send,
    recv_sem,
    chip_send,
    plane_send,
    piece_recv,
    block_send,
    block_recv,
    own_sem,
    rank_send,
    rank_recv,
):
    rows = kv_ref.shape[0]
    width = kv_ref.shape[1] // 2
    pairs = width // LANES
    tile = tops_even.shape[0]
    tiles = rows // tile
    scores, tops = (scores_even, scores_odd), (tops_even, tops_odd)
    me = lax.axis_index("ep")
    chips = lax.axis_size("ep") // CORES
    chip = me // CORES
    core = me % CORES
    other = 1 - core

    barrier = pltpu.get_barrier_semaphore()

    def loop(count, body):
        def step(index, carry):
            body(index)
            return carry

        lax.fori_loop(0, count, step, 0)

    def greet(**where):
        pl.semaphore_signal(barrier, inc=1, device_id=where)

    tp_count = lax.axis_size("tp")
    tp_me = lax.axis_index("tp")
    columns = normed_ref.shape[1] // tp_count

    def chip_at(turn):
        return lax.rem(chip + turn + 1, chips)

    def tp_at(turn):
        return lax.rem(tp_me + turn + 1, tp_count)

    ep_count = chips * CORES

    def ep_at(turn):
        return lax.rem(me + turn + 1, ep_count)

    loop(ep_count - 1, lambda turn: greet(ep=ep_at(turn)))
    loop(tp_count - 1, lambda turn: greet(tp=tp_at(turn)))
    pl.semaphore_wait(barrier, ep_count + tp_count - 2)

    def rank_copy(target, owner):
        return pltpu.make_async_remote_copy(
            src_ref=rank_ref.at[target],
            dst_ref=picks.at[owner],
            send_sem=rank_send.at[target],
            recv_sem=rank_recv.at[owner],
            device_id={"ep": target},
        )

    def up_copy(src, slot):
        return pltpu.make_async_remote_copy(
            src_ref=src,
            dst_ref=held.at[slot],
            send_sem=up_send.at[slot],
            recv_sem=recv_sem.at[slot],
            device_id={"ep": me + CORES},
        )

    def far_copy(target):
        return pltpu.make_async_remote_copy(
            src_ref=kv_ref,
            dst_ref=held.at[me],
            send_sem=up_send.at[target * CORES + core],
            recv_sem=recv_sem.at[me],
            device_id={"ep": target * CORES + core},
        )

    def side_copy(src, slot):
        return pltpu.make_async_remote_copy(
            src_ref=src,
            dst_ref=held.at[slot],
            send_sem=side_send.at[slot],
            recv_sem=recv_sem.at[slot],
            device_id={"ep": chip * CORES + other},
        )

    def lanes_of(index):
        return pl.ds(pl.multiple_of(index * columns, columns), columns)

    def chip_copy(target):
        return pltpu.make_async_remote_copy(
            src_ref=normed_ref.at[:, lanes_of(tp_me)],
            dst_ref=tokens.at[me, :, lanes_of(tp_me)],
            send_sem=chip_send.at[target],
            recv_sem=piece_recv.at[me, tp_me],
            device_id={"ep": target * CORES + core},
        )

    def plane_copy(slot, piece, target):
        place = tokens.at[slot, :, lanes_of(piece)]
        return pltpu.make_async_remote_copy(
            src_ref=place,
            dst_ref=place,
            send_sem=plane_send.at[slot, target],
            recv_sem=piece_recv.at[slot, piece],
            device_id={"tp": target},
        )

    def block_copy(src, slot):
        return pltpu.make_async_remote_copy(
            src_ref=src,
            dst_ref=tokens.at[slot],
            send_sem=block_send.at[slot],
            recv_sem=block_recv.at[slot],
            device_id={"ep": chip * CORES + other},
        )

    loop(chips - 1, lambda turn: chip_copy(chip_at(turn)).start())

    @pl.when(chip < chips - 1)
    def _():
        up_copy(kv_ref, me).start()

    reach = chips // 2
    far_count = jnp.maximum(chips - 1 - reach - chip, 0)
    loop(far_count, lambda turn: far_copy(chips - 1 - turn).start())

    @pl.when(core == 0)
    def _():
        side_copy(kv_ref, me).start()

    block_copy(normed_ref, me).start()
    own_copy = pltpu.make_async_copy(normed_ref, tokens.at[me], own_sem)
    own_copy.start()
    loop(ep_count - 1, lambda turn: rank_copy(ep_at(turn), me).start())
    picks[me] = rank_ref[me]

    def spread_pieces(turn):
        slot = chip_at(turn) * CORES + core
        plane_copy(slot, tp_me, tp_me).wait_recv()
        loop(tp_count - 1, lambda way: plane_copy(slot, tp_me, tp_at(way)).start())

    def share_blocks(turn):
        slot = chip_at(turn) * CORES + core
        loop(tp_count - 1, lambda way: plane_copy(slot, tp_at(way), tp_me).wait_recv())
        block_copy(tokens.at[slot], slot).start()

    units = [(head, index) for head in range(heads) for index in range(tiles)]
    lane = lax.broadcasted_iota(jnp.int32, (rows, LANES), 1)

    def score_unit(block, source, first, unit, slot):
        head, index = unit
        pair = head // 2
        lanes = pl.ds(pair * LANES, LANES)
        span = (index + 1) * tile if first else rows
        gates = gate_ref[pl.ds(pl.multiple_of(block * rows, rows), span), lanes]
        keys = jnp.concatenate([source[:span, lanes], gates], axis=1)
        result = lax.dot_general(
            q_ref[head, index * tile : (index + 1) * tile, :],
            keys,
            (((1,), (1,)), ((), ())),
            preferred_element_type=jnp.float32,
        )
        if first:
            q_pos = index * tile + lax.broadcasted_iota(jnp.int32, result.shape, 0)
            k_pos = lax.broadcasted_iota(jnp.int32, result.shape, 1)
            result = jnp.where(k_pos <= q_pos, result, neg_fill)
        scores[slot][:, :span] = result
        tops[slot][...] = jnp.broadcast_to(jnp.max(result, axis=1, keepdims=True), (tile, LANES))

    def value_unit(source, first, unit, slot):
        head, index = unit
        pair, part = head // 2, head % 2
        q_rows = slice(index * tile, (index + 1) * tile)
        span = (index + 1) * tile if first else rows
        new_max = tops[slot][...]
        if not first:
            old_max = row_max[head, q_rows, :]
            new_max = jnp.maximum(old_max, new_max)
        wide = jnp.concatenate([new_max] * (span // LANES), axis=1)
        probs = jnp.exp(scores[slot][:, :span] - wide).astype(jnp.bfloat16)
        values = source[:span, pl.ds(width + pair * LANES, LANES)]
        values = jnp.where(lane[:span] // HEAD == part, values, jnp.ones_like(values))
        add = jnp.dot(probs, values, preferred_element_type=jnp.float32)
        if not first:
            add = add + acc[head, q_rows, :] * jnp.exp(old_max - new_max)
        acc[head, q_rows, :] = add
        row_max[head, q_rows, :] = new_max

    def block_step(block, source, first):
        score_unit(block, source, first, units[0], 0)
        for turn, unit in enumerate(units):
            if turn + 1 < len(units):
                score_unit(block, source, first, units[turn + 1], (turn + 1) % 2)
            value_unit(source, first, unit, turn % 2)

    block_step(me, kv_ref, True)
    loop(chips - 1, spread_pieces)

    @pl.when(me == 0)
    def _():
        loop(chips - 1, share_blocks)

    def remote_step(step, carry):
        turn = step - core + 2
        own_core = turn % 2 == 0
        order = turn // 2
        back = jnp.where(order < 2, order, chip + 2 - order)
        slot = (chip - back) * CORES + jnp.where(own_core, core, other)
        landed = held.at[slot]
        side_copy(landed, slot).wait_recv()

        @pl.when(jnp.logical_and(own_core, jnp.logical_and(chip < chips - 1, back < reach)))
        def _():
            up_copy(landed, slot).start()

        @pl.when(own_core)
        def _():
            side_copy(landed, slot).start()

        @pl.when(step == jnp.maximum(me - 2, 0))
        def _():
            loop(chips - 1, share_blocks)

        block_step(slot, landed, False)
        return carry

    lax.fori_loop(0, me, remote_step, 0)

    for pair in range(pairs):
        members = []
        for head in range(2 * pair, min(2 * pair + 2, heads)):
            whole = acc[head]
            members.append(whole / pltpu.roll(whole, HEAD, 1))
        joined = members[0]
        if len(members) > 1:
            joined = jnp.where(lane < HEAD, members[0], members[1])
        count = HEAD * len(members)
        spot = slice(pair * LANES, pair * LANES + count)
        out_ref[:, spot] = joined[:, :count].astype(out_ref.dtype)

    def finish(step):
        slot = (chip - step) * CORES + core

        @pl.when(jnp.logical_and(chip < chips - 1, step < reach))
        def _():
            up_copy(held.at[slot], slot).wait_send()

        @pl.when(step > 0)
        def _():
            side_copy(held.at[slot], slot).wait_send()

    loop(chip + 1, finish)
    loop(far_count, lambda turn: far_copy(chips - 1 - turn).wait_send())

    @pl.when(core == 0)
    def _():
        side_copy(kv_ref, me).wait_send()

    def finish_tokens(turn):
        target = chip_at(turn)
        slot = target * CORES + core
        chip_copy(target).wait_send()
        loop(tp_count - 1, lambda way: plane_copy(slot, tp_me, tp_at(way)).wait_send())
        block_copy(tokens.at[slot], slot).wait_send()

    loop(chips - 1, finish_tokens)
    block_copy(normed_ref, me).wait_send()

    def finish_blocks(index):
        slot = index * CORES + other
        block_copy(tokens.at[slot], slot).wait_recv()

    loop(chips, finish_blocks)
    own_copy.wait()

    def finish_ranks(turn):
        rank_copy(ep_at(turn), me).wait_send()
        rank_copy(ep_at(turn), ep_at(turn)).wait_recv()

    loop(ep_count - 1, finish_ranks)


def exchange_kernel(count, *refs):
    sources, targets = refs[:count], refs[count : 2 * count]
    send_sem, recv_sem, own_sem = refs[2 * count :]
    tp_count = lax.axis_size("tp")
    tp_me = lax.axis_index("tp")
    barrier = pltpu.get_barrier_semaphore()
    ways = [lax.rem(tp_me + turn, tp_count) for turn in range(1, tp_count)]
    for way in ways:
        pl.semaphore_signal(barrier, inc=1, device_id={"tp": way})
    pl.semaphore_wait(barrier, tp_count - 1)

    def place(index, owner):
        span = sources[index].shape[1]
        if span % LANES:
            return targets[index].at[owner]
        return targets[index].at[:, pl.ds(pl.multiple_of(owner * span, span), span)]

    def copy(index, way, owner):
        return pltpu.make_async_remote_copy(
            src_ref=sources[index],
            dst_ref=place(index, owner),
            send_sem=send_sem.at[index, way],
            recv_sem=recv_sem.at[index, owner],
            device_id={"tp": way},
        )

    for index in range(count):
        for way in ways:
            copy(index, way, tp_me).start()
    own = [
        pltpu.make_async_copy(sources[index], place(index, tp_me), own_sem.at[index])
        for index in range(count)
    ]
    for one in own:
        one.start()
    for one in own:
        one.wait()
    for index in range(count):
        for way in ways:
            copy(index, way, way).wait_recv()
            copy(index, way, tp_me).wait_send()


def exchange(collective_id, *arrays):
    tp_count = lax.axis_size("tp")
    count = len(arrays)

    def gathered(a):
        rows, span = a.shape
        shape = (tp_count, rows, span) if span % LANES else (rows, tp_count * span)
        return jax.ShapeDtypeStruct(shape, a.dtype)

    results = pl.pallas_call(
        functools.partial(exchange_kernel, count),
        out_shape=[gathered(a) for a in arrays],
        in_specs=[pl.BlockSpec(memory_space=pltpu.VMEM)] * count,
        out_specs=[pl.BlockSpec(memory_space=pltpu.VMEM)] * count,
        scratch_shapes=[
            pltpu.SemaphoreType.DMA((count, tp_count)),
            pltpu.SemaphoreType.DMA((count, tp_count)),
            pltpu.SemaphoreType.DMA((count,)),
        ],
        compiler_params=pltpu.CompilerParams(collective_id=collective_id, has_side_effects=True),
        cost_estimate=pl.CostEstimate(flops=0, bytes_accessed=24 * 1024 * 1024, transcendentals=0),
        name="exchange",
    )(*arrays)
    return [
        r if r.ndim == 2 else r.transpose(1, 0, 2).reshape(r.shape[1], -1) for r in results
    ]


def attention(query_rows, key_rows, value_rows, cum_gate, normed, ranks):
    rows, width = query_rows.shape
    heads = width // HEAD
    pairs = (heads + 1) // 2
    ep_count = lax.axis_size("ep")
    padded = pairs * LANES
    tile = rows // 2 if rows % (2 * LANES) == 0 else rows
    if padded > width:
        spare = ((0, 0), (0, padded - width))
        query_rows, key_rows, value_rows = (
            jnp.pad(a, spare) for a in (query_rows, key_rows, value_rows)
        )
    key_value = jnp.concatenate([key_rows, value_rows], axis=1)
    scaled = query_rows * jnp.asarray(HEAD**-0.5, jnp.bfloat16)
    lane = jnp.arange(LANES)
    parts = []
    for head in range(heads):
        pair, part = head // 2, head % 2
        piece = scaled[:, pair * LANES : (pair + 1) * LANES]
        piece = jnp.where((lane // HEAD == part)[None], piece, 0)
        marks = ((lane // 3) == part).astype(jnp.bfloat16)
        parts.append(jnp.concatenate([piece, jnp.broadcast_to(marks, (rows, LANES))], axis=1))
    queries = jnp.stack(parts)
    minus = -cum_gate
    high = lax.reduce_precision(minus, 8, 7)
    rest = minus - high
    mid = lax.reduce_precision(rest, 8, 7)
    low = rest - mid
    terms = jnp.concatenate([high, mid, low], axis=0).astype(jnp.bfloat16)
    source = jnp.arange(3 * heads)
    spot = (source % heads // 2) * LANES + (source % heads % 2) * 3 + source // heads
    layout = (spot[:, None] == jnp.arange(padded)[None, :]).astype(jnp.bfloat16)
    gates = lax.dot_general(
        terms, layout, (((0,), (0,)), ((), ())), preferred_element_type=jnp.float32
    ).astype(jnp.bfloat16)
    blocks = ep_count * rows * rows * heads
    return pl.pallas_call(
        functools.partial(attention_kernel, heads),
        out_shape=[
            jax.ShapeDtypeStruct((rows, heads * HEAD), jnp.bfloat16),
            jax.ShapeDtypeStruct((ep_count,) + normed.shape, jnp.bfloat16),
            jax.ShapeDtypeStruct(ranks.shape, jnp.bfloat16),
        ],
        in_specs=[pl.BlockSpec(memory_space=pltpu.VMEM)] * 5,
        out_specs=[
            pl.BlockSpec(memory_space=pltpu.VMEM),
            pl.BlockSpec(memory_space=pl.ANY),
            pl.BlockSpec(memory_space=pltpu.VMEM),
        ],
        scratch_shapes=[
            pltpu.VMEM((ep_count, rows, 2 * padded), jnp.bfloat16),
            pltpu.VMEM((heads, rows, LANES), jnp.float32),
            pltpu.VMEM((heads, rows, LANES), jnp.float32),
            pltpu.VMEM((tile, rows), jnp.float32),
            pltpu.VMEM((tile, rows), jnp.float32),
            pltpu.VMEM((tile, LANES), jnp.float32),
            pltpu.VMEM((tile, LANES), jnp.float32),
            pltpu.SemaphoreType.DMA((ep_count,)),
            pltpu.SemaphoreType.DMA((ep_count,)),
            pltpu.SemaphoreType.DMA((ep_count,)),
            pltpu.SemaphoreType.DMA((ep_count,)),
            pltpu.SemaphoreType.DMA((ep_count, lax.axis_size("tp"))),
            pltpu.SemaphoreType.DMA((ep_count, lax.axis_size("tp"))),
            pltpu.SemaphoreType.DMA((ep_count,)),
            pltpu.SemaphoreType.DMA((ep_count,)),
            pltpu.SemaphoreType.DMA,
            pltpu.SemaphoreType.DMA((ep_count,)),
            pltpu.SemaphoreType.DMA((ep_count,)),
        ],
        compiler_params=pltpu.CompilerParams(
            collective_id=0, has_side_effects=True, vmem_limit_bytes=48 * 1024 * 1024
        ),
        cost_estimate=pl.CostEstimate(
            flops=blocks * 2 * 512, bytes_accessed=8 * 1024 * 1024, transcendentals=blocks
        ),
        name="attend",
    )(queries, key_value, gates, normed, ranks)


def local(
    query_rows,
    key_rows,
    value_rows,
    cum_gate,
    out_weight,
    moe_input,
    moe_gain,
    routes,
    route_weight,
    expert_gate,
    expert_up,
    expert_down,
    shared_gate,
    shared_up,
    shared_down,
):
    token_count = moe_input.shape[0]
    top_count = routes.shape[1]
    local_experts = expert_gate.shape[0]
    ep_count = lax.axis_size("ep")
    expert_count = local_experts * ep_count
    capacity = 2 * token_count * top_count // expert_count
    column_count = expert_down.shape[2]
    first_column = lax.axis_index("tp") * column_count
    moe_rows = moe_input.astype(jnp.float32)
    normed = (
        moe_rows
        * lax.rsqrt(jnp.mean(moe_rows * moe_rows, axis=1, keepdims=True) + norm_eps)
        * moe_gain
    ).astype(jnp.bfloat16)
    expert_ids = jnp.arange(expert_count, dtype=jnp.int32)
    chosen = routes[:, :, None] == expert_ids[None, None, :]
    named = jnp.any(chosen, axis=1)
    weight_of = jnp.sum(jnp.where(chosen, route_weight[:, :, None], 0.0), axis=1)
    order = jnp.arange(token_count)
    earlier = (order[None, :] < order[:, None]).astype(jnp.bfloat16)
    ranks = jnp.dot(earlier, named.astype(jnp.bfloat16), preferred_element_type=jnp.float32)
    ranks = jnp.where(named, ranks.astype(jnp.int32), -1)
    slots = jnp.arange(capacity, dtype=jnp.int32)
    place = ranks[:, :, None] == slots[None, None, :]
    rank_rows = ranks.astype(jnp.bfloat16).T.reshape(ep_count, local_experts, token_count)
    heads_out, tokens, mine = attention(
        query_rows, key_rows, value_rows, cum_gate, normed, rank_rows
    )
    pick = mine[:, :, None, :] == slots.astype(jnp.bfloat16)[None, None, :, None]
    pick = pick.astype(jnp.bfloat16).reshape(ep_count, local_experts * capacity, token_count)
    arrived = jnp.einsum("ast,atd->asd", pick, tokens, preferred_element_type=jnp.float32)
    arrived = arrived.astype(jnp.bfloat16).reshape(ep_count, local_experts, capacity, -1)
    gate_val = jnp.einsum(
        "aecd,edf->aecf", arrived, expert_gate, preferred_element_type=jnp.float32
    )
    up_val = jnp.einsum("aecd,edf->aecf", arrived, expert_up, preferred_element_type=jnp.float32)
    hidden = (jax.nn.silu(gate_val) * up_val).astype(jnp.bfloat16)
    shared_hidden = (
        jax.nn.silu(jnp.dot(normed, shared_gate, preferred_element_type=jnp.float32))
        * jnp.dot(normed, shared_up, preferred_element_type=jnp.float32)
    ).astype(jnp.bfloat16)
    slot_count = ep_count * local_experts * capacity
    by_expert = hidden.transpose(1, 0, 2, 3).reshape(slot_count, hidden.shape[3])
    hidden, shared_all = exchange(1, by_expert, shared_hidden)
    hidden = hidden.reshape(local_experts, ep_count * capacity, -1)
    result = jnp.einsum("esf,efd->esd", hidden, expert_down, preferred_element_type=jnp.float32)
    result = result.astype(jnp.bfloat16).reshape(local_experts, ep_count, capacity, column_count)
    result = result.transpose(1, 0, 2, 3)
    result, heads_out = lax.optimization_barrier((result, heads_out))
    returned = lax.all_to_all(result, "ep", split_axis=0, concat_axis=0, tiled=True)
    returned = returned.reshape(expert_count * capacity, column_count)
    weight_high = lax.reduce_precision(weight_of, 8, 7)
    weight_low = weight_of - weight_high
    routed = 0.0
    for weight in (weight_high, weight_low):
        spread = jnp.where(place, weight[:, :, None], 0.0).astype(jnp.bfloat16)
        routed = routed + jnp.dot(
            spread.reshape(token_count, expert_count * capacity),
            returned,
            preferred_element_type=jnp.float32,
        )
    (heads_all,) = exchange(2, heads_out)
    mixer_sum = jnp.dot(heads_all, out_weight, preferred_element_type=jnp.float32)
    moe_total = routed + jnp.dot(shared_all, shared_down, preferred_element_type=jnp.float32)
    return (mixer_sum.astype(jnp.bfloat16), moe_total.astype(jnp.bfloat16))


def solution(mesh):
    placed = (
        P("ep", "tp"),
        P("ep", "tp"),
        P("ep", "tp"),
        P("tp", None),
        P(None, "tp"),
        P("ep", None),
        P(),
        P("ep", None),
        P("ep", None),
        P("ep", None, "tp"),
        P("ep", None, "tp"),
        P("ep", None, "tp"),
        P(None, "tp"),
        P(None, "tp"),
        P(None, "tp"),
    )
    return jax.shard_map(
        local, mesh=mesh, in_specs=placed, out_specs=(P("ep", "tp"), P("ep", "tp")), check_vma=False
    )
```

```python
import functools

import jax
import jax.numpy as jnp
from jax import lax
from jax.experimental import pallas as pl
from jax.experimental.pallas import tpu as pltpu
from jax.sharding import PartitionSpec as P

HEAD = 64
LANES = 128
CORES = 2
ROW_TILE = 16

neg_fill = -1e30
norm_eps = 1e-06


def silu_mul(both):
    gate, up = both[:, :LANES], both[:, LANES:]
    return (gate / (1.0 + jnp.exp(-gate)) * up).astype(jnp.bfloat16)


def block_kernel(
    heads,
    main,
    tail,
    q_hbm,
    k_hbm,
    v_hbm,
    gate_ref,
    normed_ref,
    rank_ref,
    expert_gate,
    expert_up,
    expert_down,
    shared_gate,
    shared_up,
    heads_all,
    returned,
    shared_all,
    tokens,
    q_own,
    q_guest,
    held,
    acc,
    row_max,
    guest_acc,
    guest_max,
    guest_out,
    guest_in,
    guest_lse,
    lse_in,
    scores_even,
    scores_odd,
    tops_even,
    tops_odd,
    picks,
    staged,
    arrived,
    gate_up,
    down,
    shared_both,
    hidden,
    results,
    load_sem,
    up_send,
    side_send,
    kv_recv,
    guest_send,
    guest_recv,
    chip_send,
    plane_send,
    piece_recv,
    block_send,
    block_recv,
    rank_send,
    rank_recv,
    shared_send,
    shared_recv,
    hidden_send,
    hidden_recv,
    heads_send,
    heads_recv,
    result_send,
    result_recv,
    stage_sem,
):
    ep_slots, pairs, _, rows, _ = held.shape
    group = min(2, heads)
    experts = expert_gate.shape[0]
    tile = tops_even.shape[0]
    tiles = rows // tile
    scores, tops = (scores_even, scores_odd), (tops_even, tops_odd)
    me = lax.axis_index("ep")
    ep_count = lax.axis_size("ep")
    chips = ep_count // CORES
    chip = me // CORES
    core = me % CORES
    other = 1 - core
    tp_count = lax.axis_size("tp")
    tp_me = lax.axis_index("tp")
    columns = normed_ref.shape[1] // tp_count
    last = chips - 1
    host = chips - 2
    guests = chips > 2

    barrier = pltpu.get_barrier_semaphore()

    def loop(count, body):
        def step(index, carry):
            body(index)
            return carry

        lax.fori_loop(0, count, step, 0)

    def greet(**where):
        pl.semaphore_signal(barrier, inc=1, device_id=where)

    def chip_at(turn):
        return lax.rem(chip + turn + 1, chips)

    def tp_at(turn):
        return lax.rem(tp_me + turn + 1, tp_count)

    def ep_at(turn):
        return lax.rem(me + turn + 1, ep_count)

    def lanes_at(index, width):
        return pl.ds(pl.multiple_of(index * width, width), width)

    loads = [
        pltpu.make_async_copy(q_hbm, q_own, load_sem.at[0]),
    ]
    for pair in range(pairs):
        lanes = pl.ds(pair * LANES, LANES)
        for part, source in enumerate((k_hbm, v_hbm)):
            loads.append(
                pltpu.make_async_copy(
                    source.at[:, lanes],
                    held.at[me, pair, part],
                    load_sem.at[len(loads)],
                )
            )
    weights = []
    for source, place in (
        (shared_gate, shared_both.at[:, pl.ds(0, LANES)]),
        (shared_up, shared_both.at[:, pl.ds(LANES, LANES)]),
        (expert_gate, gate_up.at[:, :, pl.ds(0, LANES)]),
        (expert_up, gate_up.at[:, :, pl.ds(LANES, LANES)]),
        (expert_down, down),
    ):
        index = len(loads) + len(weights)
        weights.append(pltpu.make_async_copy(source, place, load_sem.at[index]))
    for one in loads + weights:
        one.start()

    loop(ep_count - 1, lambda turn: greet(ep=ep_at(turn)))
    loop(tp_count - 1, lambda turn: greet(tp=tp_at(turn)))
    pl.semaphore_wait(barrier, ep_count + tp_count - 2)

    def remote(source, target, send, recv, **where):
        return pltpu.make_async_remote_copy(
            src_ref=source, dst_ref=target, send_sem=send, recv_sem=recv, device_id=where
        )

    def rank_copy(target, owner):
        return remote(
            rank_ref.at[target], picks.at[owner], rank_send.at[target], rank_recv.at[owner], ep=target
        )

    def up_copy(slot, pair):
        place = held.at[slot, pair]
        return remote(place, place, up_send.at[slot, pair], kv_recv.at[slot, pair], ep=me + CORES)

    def side_copy(slot, pair):
        place = held.at[slot, pair]
        return remote(
            place, place, side_send.at[slot, pair], kv_recv.at[slot, pair], ep=chip * CORES + other
        )

    def guest_query(pair):
        lanes = lanes_at(pair, LANES)
        return remote(
            q_own.at[:, lanes],
            q_guest.at[:, lanes],
            guest_send.at[0, pair],
            guest_recv.at[0, pair],
            ep=me - CORES,
        )

    def guest_result(pair):
        return remote(
            guest_out.at[pair],
            guest_in.at[pair],
            guest_send.at[1, pair],
            guest_recv.at[1, pair],
            ep=me + CORES,
        )

    def guest_stats(pair):
        return remote(
            guest_lse.at[pair],
            lse_in.at[pair],
            guest_send.at[2, pair],
            guest_recv.at[2, pair],
            ep=me + CORES,
        )

    def chip_copy(target):
        return remote(
            normed_ref.at[:, lanes_at(tp_me, columns)],
            tokens.at[me, :, lanes_at(tp_me, columns)],
            chip_send.at[target],
            piece_recv.at[me, tp_me],
            ep=target * CORES + core,
        )

    def plane_copy(slot, piece, target):
        place = tokens.at[slot, :, lanes_at(piece, columns)]
        return remote(
            place, place, plane_send.at[slot, target], piece_recv.at[slot, piece], tp=target
        )

    def block_copy(source, slot):
        return remote(
            source,
            tokens.at[slot],
            block_send.at[slot],
            block_recv.at[slot],
            ep=chip * CORES + other,
        )

    def shared_copy(owner, target):
        place = shared_all.at[owner]
        return remote(place, place, shared_send.at[target], shared_recv.at[owner], tp=target)

    def hidden_copy(owner, target):
        place = hidden.at[owner]
        return remote(place, place, hidden_send.at[target], hidden_recv.at[owner], tp=target)

    wide_heads = heads * HEAD % LANES == 0

    def heads_place(owner, pair):
        if wide_heads:
            return heads_all.at[:, lanes_at(owner * pairs + pair, LANES)]
        return heads_all.at[owner]

    def heads_copy(owner, pair, target):
        place = heads_place(owner, pair)
        return remote(
            place, place, heads_send.at[pair, target], heads_recv.at[pair, owner], tp=target
        )

    def result_copy(target, owner):
        return remote(
            results.at[target],
            returned.at[owner],
            result_send.at[target],
            result_recv.at[owner],
            ep=target,
        )

    loop(ep_count - 1, lambda turn: rank_copy(ep_at(turn), me).start())
    loop(chips - 1, lambda turn: chip_copy(chip_at(turn)).start())
    block_copy(normed_ref, me).start()
    picks[me] = rank_ref[me]
    for one in loads:
        one.wait()

    for pair in range(pairs):

        @pl.when(chip < last)
        def _():
            up_copy(me, pair).start()

        @pl.when(core == 0)
        def _():
            side_copy(me, pair).start()

        if guests:

            @pl.when(chip == last)
            def _():
                guest_query(pair).start()

    units = [(member, index) for member in range(group) for index in range(tiles)]
    lane = lax.broadcasted_iota(jnp.int32, (rows, LANES), 1)
    scale = jnp.asarray(HEAD**-0.5, jnp.bfloat16)

    def attend(pair, slot, queries, sums, maxima, first):
        def score_unit(unit, way):
            member, index = unit
            span = (index + 1) * tile if first else rows
            query = queries[index * tile : (index + 1) * tile, lanes_at(pair, LANES)] * scale
            query = jnp.where(lane[:tile] // HEAD == member, query, jnp.zeros_like(query))
            gates = gate_ref[pair * group + member, :, lanes_at(slot, rows)]
            result = lax.dot_general(
                query,
                held[slot, pair, 0, :span, :],
                (((1,), (1,)), ((), ())),
                preferred_element_type=jnp.float32,
            )
            result = result - gates[:, :span]
            if first:
                q_pos = index * tile + lax.broadcasted_iota(jnp.int32, result.shape, 0)
                k_pos = lax.broadcasted_iota(jnp.int32, result.shape, 1)
                result = jnp.where(k_pos <= q_pos, result, neg_fill)
            scores[way][:, :span] = result
            top = jnp.max(result, axis=1, keepdims=True)
            tops[way][...] = jnp.broadcast_to(top, (tile, LANES))

        def value_unit(unit, way):
            member, index = unit
            head = pair * group + member
            q_rows = slice(index * tile, (index + 1) * tile)
            span = (index + 1) * tile if first else rows
            new_max = tops[way][...]
            if not first:
                old_max = maxima[head, q_rows, :]
                new_max = jnp.maximum(old_max, new_max)
            wide = jnp.concatenate([new_max] * (span // LANES), axis=1)
            probs = jnp.exp(scores[way][:, :span] - wide).astype(jnp.bfloat16)
            values = held[slot, pair, 1, :span, :]
            values = jnp.where(lane[:span] // HEAD == member, values, jnp.ones_like(values))
            add = jnp.dot(probs, values, preferred_element_type=jnp.float32)
            if not first:
                add = add + sums[head, q_rows, :] * jnp.exp(old_max - new_max)
            sums[head, q_rows, :] = add
            maxima[head, q_rows, :] = new_max

        score_unit(units[0], 0)
        for turn, unit in enumerate(units):
            if turn + 1 < len(units):
                score_unit(units[turn + 1], (turn + 1) % 2)
            value_unit(unit, turn % 2)

    def spread_pieces(turn):
        slot = chip_at(turn) * CORES + core
        plane_copy(slot, tp_me, tp_me).wait_recv()
        loop(tp_count - 1, lambda way: plane_copy(slot, tp_me, tp_at(way)).start())

    def share_blocks(turn):
        slot = chip_at(turn) * CORES + core
        loop(tp_count - 1, lambda way: plane_copy(slot, tp_at(way), tp_me).wait_recv())
        block_copy(tokens.at[slot], slot).start()

    def shared_stage():
        for one in weights[:2]:
            one.wait()
        both = jnp.dot(normed_ref[...], shared_both[...], preferred_element_type=jnp.float32)
        shared_all[tp_me] = silu_mul(both)
        loop(tp_count - 1, lambda way: shared_copy(tp_me, tp_at(way)).start())

    token_count = normed_ref.shape[0]
    slot_rows = arrived.shape[1]
    tail_rows = slot_rows - experts * main
    tail_at = experts * main

    def gather_block(slot, block):
        ranks = picks[slot].astype(jnp.float32)
        parts = []
        if main:
            order = lax.broadcasted_iota(jnp.int32, (main, token_count), 0).astype(jnp.float32)
            for expert in range(experts):
                hit = ranks[expert : expert + 1, :] == order
                parts.append(jnp.where(hit, 1.0, 0.0))
        if tail_rows:
            order = lax.broadcasted_iota(jnp.int32, (tail_rows, token_count), 0)
            found = jnp.zeros((tail_rows, token_count), jnp.float32)
            for expert in range(experts):
                begin = expert * tail
                wanted = (order - begin + main).astype(jnp.float32)
                hit = ranks[expert : expert + 1, :] == wanted
                inside = jnp.logical_and(order >= begin, order < begin + tail)
                found = jnp.where(jnp.logical_and(hit, inside), 1.0, found)
            parts.append(found)
        pick = jnp.concatenate(parts, axis=0).astype(jnp.bfloat16)
        rows_in = jnp.dot(pick, block, preferred_element_type=jnp.float32)
        arrived[slot] = rows_in.astype(jnp.bfloat16)

    def tail_select(value_of, width):
        order = lax.broadcasted_iota(jnp.int32, (ep_slots, tail_rows, width), 1)
        order = order.reshape(ep_slots * tail_rows, width)
        total = value_of(0)
        for expert in range(1, experts):
            total = jnp.where(order >= expert * tail, value_of(expert), total)
        return total

    def up_stage():
        own_block = pltpu.make_async_copy(normed_ref, tokens.at[me], stage_sem.at[0])
        own_block.start()

        def finish_blocks(index):
            slot = index * CORES + other
            block_copy(tokens.at[slot], slot).wait_recv()

        def finish_ranks(turn):
            rank_copy(ep_at(turn), ep_at(turn)).wait_recv()

        own_block.wait()
        loop(ep_count - 1, finish_ranks)
        loop(chips, finish_blocks)

        def gather(slot):
            if staged is None:
                gather_block(slot, tokens[slot])
            else:
                fetch = pltpu.make_async_copy(tokens.at[slot], staged, stage_sem.at[1])
                fetch.start()
                fetch.wait()
                gather_block(slot, staged[...])

        loop(ep_count, gather)
        for one in weights[2:4]:
            one.wait()
        depth = arrived.shape[2]
        if main:

            def expert_step(expert):
                span = pl.ds(pl.multiple_of(expert * main, main), main)
                block = arrived[:, span, :].reshape(ep_slots * main, depth)
                both = jnp.dot(block, gate_up[expert], preferred_element_type=jnp.float32)
                hidden[tp_me, :, span, :] = silu_mul(both).reshape(ep_slots, main, LANES)

            loop(experts, expert_step)
        if tail_rows:
            block = arrived[:, tail_at:, :].reshape(ep_slots * tail_rows, depth)
            both = tail_select(
                lambda e: jnp.dot(block, gate_up[e], preferred_element_type=jnp.float32),
                2 * LANES,
            )
            hidden[tp_me, :, tail_at:, :] = silu_mul(both).reshape(ep_slots, tail_rows, LANES)
        loop(tp_count - 1, lambda way: hidden_copy(tp_me, tp_at(way)).start())

    def down_stage():
        weights[4].wait()
        loop(tp_count - 1, lambda way: hidden_copy(tp_at(way), tp_at(way)).wait_recv())
        width = down.shape[2]

        def joined(span, count):
            parts = [
                hidden[piece, :, span, :].reshape(ep_slots * count, LANES)
                for piece in range(tp_count)
            ]
            return jnp.concatenate(parts, axis=1)

        if main:

            def expert_step(expert):
                span = pl.ds(pl.multiple_of(expert * main, main), main)
                out = jnp.dot(joined(span, main), down[expert], preferred_element_type=jnp.float32)
                results[:, span, :] = out.astype(jnp.bfloat16).reshape(ep_slots, main, width)

            loop(experts, expert_step)
        if tail_rows:
            block = joined(pl.ds(tail_at, tail_rows), tail_rows)
            out = tail_select(
                lambda e: jnp.dot(block, down[e], preferred_element_type=jnp.float32), width
            )
            out = out.astype(jnp.bfloat16).reshape(ep_slots, tail_rows, width)
            results[:, tail_at:, :] = out
        loop(ep_count - 1, lambda turn: result_copy(ep_at(turn), me).start())
        returned[me] = results[me]

    def ratio(sums, head):
        whole = sums[head]
        return whole / pltpu.roll(whole, HEAD, 1)

    def pair_out(sums, pair):
        joined = ratio(sums, pair * group)
        if group > 1:
            joined = jnp.where(lane < HEAD, joined, ratio(sums, pair * group + 1))
        return joined.astype(jnp.bfloat16)

    def send_guest(pair):
        guest_out[pair] = pair_out(guest_acc, pair)
        stats = jnp.zeros((rows, LANES), jnp.float32)
        for member in range(group):
            whole = guest_acc[pair * group + member]
            total = jnp.where(lane // HEAD == member, pltpu.roll(whole, HEAD, 1), whole)
            value = guest_max[pair * group + member] + jnp.log(total)
            stats = jnp.where(lane == member, value, stats)
        guest_lse[pair] = stats.T[:8, :]
        guest_result(pair).start()
        guest_stats(pair).start()

    def merge_guest(pair):
        guest_result(pair).wait_recv()
        guest_stats(pair).wait_recv()
        stats = jnp.concatenate([lse_in[pair]] * (LANES // 8), axis=0).T
        outer = guest_in[pair].astype(jnp.float32)
        for member in range(group):
            head = pair * group + member
            value = jnp.broadcast_to(stats[:, member : member + 1], (rows, LANES))
            new_max = jnp.maximum(row_max[head], value)
            part = jnp.where(lane // HEAD == member, outer, 1.0)
            acc[head] = acc[head] * jnp.exp(row_max[head] - new_max) + part * jnp.exp(
                value - new_max
            )

    def finish_pair(pair):
        if guests:

            @pl.when(chip == last)
            def _():
                merge_guest(pair)

        if wide_heads:
            heads_all[:, lanes_at(tp_me * pairs + pair, LANES)] = pair_out(acc, pair)
        else:
            heads_all[tp_me] = pair_out(acc, pair)
        loop(tp_count - 1, lambda way: heads_copy(tp_me, pair, tp_at(way)).start())

    reach = 1 if guests else chips
    deepest = jnp.where(chip == last, jnp.minimum(chip, reach), chip)
    step_count = deepest * CORES + core
    turns = 1 + max(CORES * (host if guests else last) + 1, CORES + 1)
    delay = 3 if guests else 0
    total = pairs * turns

    def remote_step(pair, step):
        turn = step - core + CORES
        own_core = turn % CORES == 0
        back = turn // CORES
        slot = (chip - back) * CORES + jnp.where(own_core, core, other)
        side_copy(slot, pair).wait_recv()

        @pl.when(jnp.logical_and(own_core, chip < (host if guests else last)))
        def _():
            up_copy(slot, pair).start()

        @pl.when(own_core)
        def _():
            side_copy(slot, pair).start()

        attend(pair, slot, q_own, acc, row_max, False)
        if guests:

            @pl.when(jnp.logical_and(chip == host, back >= 1))
            def _():
                @pl.when(step == core)
                def _():
                    guest_query(pair).wait_recv()
                    for member in range(group):
                        head = pair * group + member
                        guest_acc[head] = jnp.zeros((rows, LANES), jnp.float32)
                        guest_max[head] = jnp.full((rows, LANES), neg_fill, jnp.float32)

                attend(pair, slot, q_guest, guest_acc, guest_max, False)

    share_at = chips
    up_at = chips + 1
    down_at = total - 3

    def one_turn(index):
        pair = index // turns
        turn = index % turns

        @pl.when(jnp.logical_and(index >= 1, index < chips))
        def _():
            spread_pieces(index - 1)

        @pl.when(index == 1)
        def _():
            shared_stage()

        @pl.when(index == share_at)
        def _():
            loop(chips - 1, share_blocks)

        @pl.when(index == up_at)
        def _():
            up_stage()

        @pl.when(index == down_at)
        def _():
            down_stage()

        @pl.when(index < total)
        def _():
            @pl.when(turn == 0)
            def _():
                attend(pair, me, q_own, acc, row_max, True)

            @pl.when(jnp.logical_and(turn >= 1, turn <= step_count))
            def _():
                remote_step(pair, turn - 1)

            if guests:

                @pl.when(jnp.logical_and(chip == host, turn == turns - 1))
                def _():
                    send_guest(pair)

        late = index - jnp.where(chip == last, delay, 0)

        @pl.when(jnp.logical_and(late >= 0, late % turns == turns - 1))
        def _():
            @pl.when(late < total)
            def _():
                finish_pair(late // turns)

    loop(total + delay, one_turn)

    for pair in range(pairs):

        def finish_kv(back):
            slot = (chip - back) * CORES + core

            @pl.when(
                jnp.logical_or(
                    chip < (host if guests else last), jnp.logical_and(back == 0, chip < last)
                )
            )
            def _():
                up_copy(slot, pair).wait_send()

            @pl.when(back > 0)
            def _():
                side_copy(slot, pair).wait_send()

        loop(deepest + 1, finish_kv)

        @pl.when(core == 0)
        def _():
            side_copy(me, pair).wait_send()

        if guests:

            @pl.when(chip == last)
            def _():
                guest_query(pair).wait_send()

            @pl.when(chip == host)
            def _():
                guest_result(pair).wait_send()
                guest_stats(pair).wait_send()

    def finish_tokens(turn):
        target = chip_at(turn)
        slot = target * CORES + core
        chip_copy(target).wait_send()
        loop(tp_count - 1, lambda way: plane_copy(slot, tp_me, tp_at(way)).wait_send())
        block_copy(tokens.at[slot], slot).wait_send()

    loop(chips - 1, finish_tokens)
    block_copy(normed_ref, me).wait_send()

    def finish_peers(turn):
        rank_copy(ep_at(turn), me).wait_send()
        result_copy(ep_at(turn), me).wait_send()
        result_copy(ep_at(turn), ep_at(turn)).wait_recv()

    loop(ep_count - 1, finish_peers)

    def finish_plane(way):
        peer = tp_at(way)
        shared_copy(tp_me, peer).wait_send()
        shared_copy(peer, peer).wait_recv()
        hidden_copy(tp_me, peer).wait_send()
        for pair in range(pairs):
            heads_copy(tp_me, pair, peer).wait_send()
            heads_copy(peer, pair, peer).wait_recv()

    loop(tp_count - 1, finish_plane)


def slot_layout(capacity, experts):
    main = capacity // ROW_TILE * ROW_TILE
    tail = capacity - main
    tail_rows = -(-tail * experts // ROW_TILE) * ROW_TILE
    return main, tail, experts * main + tail_rows


def padded(a, axis, to):
    if a.shape[axis] == to:
        return a
    spare = [(0, 0)] * a.ndim
    spare[axis] = (0, to - a.shape[axis])
    return jnp.pad(a, spare)


def fused_block(
    query_rows,
    key_rows,
    value_rows,
    cum_gate,
    normed,
    ranks,
    capacity,
    expert_gate,
    expert_up,
    expert_down,
    shared_gate,
    shared_up,
):
    rows, width = query_rows.shape
    heads = width // HEAD
    pairs = (heads + 1) // 2
    ep_count = lax.axis_size("ep")
    tp_count = lax.axis_size("tp")
    chips = ep_count // CORES
    lanes = pairs * LANES
    tile = rows // 2 if rows % (2 * LANES) == 0 else rows
    query_rows, key_rows, value_rows = (
        padded(a, 1, lanes) for a in (query_rows, key_rows, value_rows)
    )
    experts, depth, span = expert_gate.shape
    columns = expert_down.shape[2]
    token_count = normed.shape[0]
    main, tail, slot_rows = slot_layout(capacity, experts)
    if span < LANES:
        expert_gate, expert_up = padded(expert_gate, 2, LANES), padded(expert_up, 2, LANES)
        shared_gate, shared_up = padded(shared_gate, 1, LANES), padded(shared_up, 1, LANES)
        expert_down = padded(expert_down.reshape(experts, tp_count, span, columns), 2, LANES)
        expert_down = expert_down.reshape(experts, tp_count * LANES, columns)
    inside = ep_count * token_count * depth * 2 <= 8 * 1024 * 1024
    bf16, f32 = jnp.bfloat16, jnp.float32
    vmem = pl.BlockSpec(memory_space=pltpu.VMEM)
    anywhere = pl.BlockSpec(memory_space=pl.ANY)
    heads_shape = (rows, tp_count * width) if width % LANES == 0 else (tp_count, rows, LANES)
    outs = [
        jax.ShapeDtypeStruct(heads_shape, bf16),
        jax.ShapeDtypeStruct((ep_count, slot_rows, columns), bf16),
        jax.ShapeDtypeStruct((tp_count, token_count, LANES), bf16),
    ]
    out_specs = [vmem] * 3
    token_shape = (ep_count, token_count, depth)
    scratch = []
    if inside:
        scratch.append(pltpu.VMEM(token_shape, bf16))
    else:
        outs.append(jax.ShapeDtypeStruct(token_shape, bf16))
        out_specs.append(anywhere)
    dma = pltpu.SemaphoreType.DMA
    scratch += [
        pltpu.VMEM((rows, lanes), bf16),
        pltpu.VMEM((rows, lanes), bf16),
        pltpu.VMEM((ep_count, pairs, 2, rows, LANES), bf16),
        pltpu.VMEM((heads, rows, LANES), f32),
        pltpu.VMEM((heads, rows, LANES), f32),
        pltpu.VMEM((heads, rows, LANES), f32),
        pltpu.VMEM((heads, rows, LANES), f32),
        pltpu.VMEM((pairs, rows, LANES), bf16),
        pltpu.VMEM((pairs, rows, LANES), bf16),
        pltpu.VMEM((pairs, 8, rows), f32),
        pltpu.VMEM((pairs, 8, rows), f32),
        pltpu.VMEM((tile, rows), f32),
        pltpu.VMEM((tile, rows), f32),
        pltpu.VMEM((tile, LANES), f32),
        pltpu.VMEM((tile, LANES), f32),
        pltpu.VMEM(ranks.shape, bf16),
    ]
    if not inside:
        scratch.append(pltpu.VMEM((token_count, depth), bf16))
    scratch += [
        pltpu.VMEM((ep_count, slot_rows, depth), bf16),
        pltpu.VMEM((experts, depth, 2 * LANES), bf16),
        pltpu.VMEM(expert_down.shape, bf16),
        pltpu.VMEM((depth, 2 * LANES), bf16),
        pltpu.VMEM((tp_count, ep_count, slot_rows, LANES), bf16),
        pltpu.VMEM((ep_count, slot_rows, columns), bf16),
        dma((6 + 2 * pairs,)),
        dma((ep_count, pairs)),
        dma((ep_count, pairs)),
        dma((ep_count, pairs)),
        dma((3, pairs)),
        dma((3, pairs)),
        dma((chips,)),
        dma((ep_count, tp_count)),
        dma((ep_count, tp_count)),
        dma((ep_count,)),
        dma((ep_count,)),
        dma((ep_count,)),
        dma((ep_count,)),
        dma((tp_count,)),
        dma((tp_count,)),
        dma((tp_count,)),
        dma((tp_count,)),
        dma((pairs, tp_count)),
        dma((pairs, tp_count)),
        dma((ep_count,)),
        dma((ep_count,)),
        dma((2,)),
    ]
    body = functools.partial(block_kernel, heads, main, tail)
    inputs = 11

    def kernel(*refs):
        refs = list(refs)
        if inside:
            refs.insert(inputs + 3 + 17, None)
        body(*refs)

    blocks = ep_count * rows * rows * heads
    results = pl.pallas_call(
        kernel,
        out_shape=outs,
        in_specs=[anywhere] * 3 + [vmem] * 3 + [anywhere] * 5,
        out_specs=out_specs,
        scratch_shapes=scratch,
        compiler_params=pltpu.CompilerParams(
            collective_id=0, has_side_effects=True, vmem_limit_bytes=58 * 1024 * 1024
        ),
        cost_estimate=pl.CostEstimate(
            flops=blocks * 2 * 512, bytes_accessed=8 * 1024 * 1024, transcendentals=blocks
        ),
        name="fused_block",
    )(
        query_rows,
        key_rows,
        value_rows,
        cum_gate[:, None, :],
        normed,
        ranks,
        expert_gate,
        expert_up,
        expert_down,
        shared_gate,
        shared_up,
    )
    heads_all, returned, shared_all = results[:3]
    if heads_all.ndim == 3:
        heads_all = heads_all[:, :, :width].transpose(1, 0, 2).reshape(rows, -1)
    shared_all = shared_all[:, :, :span].transpose(1, 0, 2).reshape(token_count, -1)
    return heads_all, returned, shared_all


def local(
    query_rows,
    key_rows,
    value_rows,
    cum_gate,
    out_weight,
    moe_input,
    moe_gain,
    routes,
    route_weight,
    expert_gate,
    expert_up,
    expert_down,
    shared_gate,
    shared_up,
    shared_down,
):
    token_count = moe_input.shape[0]
    top_count = routes.shape[1]
    local_experts = expert_gate.shape[0]
    ep_count = lax.axis_size("ep")
    expert_count = local_experts * ep_count
    capacity = 2 * token_count * top_count // expert_count
    moe_rows = moe_input.astype(jnp.float32)
    normed = (
        moe_rows
        * lax.rsqrt(jnp.mean(moe_rows * moe_rows, axis=1, keepdims=True) + norm_eps)
        * moe_gain
    ).astype(jnp.bfloat16)
    expert_ids = jnp.arange(expert_count, dtype=jnp.int32)
    chosen = routes[:, :, None] == expert_ids[None, None, :]
    named = jnp.any(chosen, axis=1)
    order = jnp.arange(token_count)
    earlier = (order[None, :] < order[:, None]).astype(jnp.bfloat16)
    ranks = jnp.dot(earlier, named.astype(jnp.bfloat16), preferred_element_type=jnp.float32)
    ranks = jnp.where(named, ranks.astype(jnp.int32), -1)
    rank_rows = ranks.astype(jnp.bfloat16).T.reshape(ep_count, local_experts, token_count)
    heads_all, returned, shared_all = fused_block(
        query_rows,
        key_rows,
        value_rows,
        cum_gate,
        normed,
        rank_rows,
        capacity,
        expert_gate,
        expert_up,
        expert_down,
        shared_gate,
        shared_up,
    )
    main, tail, slot_rows = slot_layout(capacity, local_experts)
    taken = jnp.sum(jnp.where(chosen, ranks[:, None, :], 0), axis=2)
    local_id = routes % local_experts
    spot = jnp.where(
        taken < main,
        local_id * main + taken,
        local_experts * main + local_id * tail + taken - main,
    )
    spot = spot + routes // local_experts * slot_rows
    spots = jnp.arange(ep_count * slot_rows, dtype=jnp.int32)
    weight = jnp.zeros((token_count, ep_count * slot_rows), jnp.float32)
    for choice in range(top_count):
        hit = spot[:, choice : choice + 1] == spots[None, :]
        weight = jnp.where(hit, route_weight[:, choice : choice + 1], weight)
    weight_high = lax.reduce_precision(weight, 8, 7)
    weight_low = weight - weight_high
    results = returned.reshape(ep_count * slot_rows, -1)
    moe_total = jnp.dot(shared_all, shared_down, preferred_element_type=jnp.float32)
    for part in (weight_high, weight_low):
        moe_total = moe_total + jnp.dot(
            part.astype(jnp.bfloat16), results, preferred_element_type=jnp.float32
        )
    mixer_sum = jnp.dot(heads_all, out_weight, preferred_element_type=jnp.float32)
    return (mixer_sum.astype(jnp.bfloat16), moe_total.astype(jnp.bfloat16))


def solution(mesh):
    placed = (
        P("ep", "tp"),
        P("ep", "tp"),
        P("ep", "tp"),
        P("tp", None),
        P(None, "tp"),
        P("ep", None),
        P(),
        P("ep", None),
        P("ep", None),
        P("ep", None, "tp"),
        P("ep", None, "tp"),
        P("ep", None, "tp"),
        P(None, "tp"),
        P(None, "tp"),
        P(None, "tp"),
    )
    return jax.shard_map(
        local, mesh=mesh, in_specs=placed, out_specs=(P("ep", "tp"), P("ep", "tp")), check_vma=False
    )
```

```python
import functools

import jax
import jax.numpy as jnp
from jax import lax
from jax.experimental import pallas as pl
from jax.experimental.pallas import tpu as pltpu
from jax.sharding import PartitionSpec as P

HEAD = 64
LANES = 128
CORES = 2
ROW_TILE = 16

neg_fill = -1e30
norm_eps = 1e-06


def silu_mul(both):
    gate, up = both[:, :LANES], both[:, LANES:]
    return (gate / (1.0 + jnp.exp(-gate)) * up).astype(jnp.bfloat16)


def block_kernel(
    heads,
    main,
    tail,
    q_hbm,
    k_hbm,
    v_hbm,
    gate_ref,
    routes_ref,
    weight_ref,
    gain_ref,
    moe_hbm,
    expert_gate,
    expert_up,
    expert_down,
    shared_gate,
    shared_up,
    shared_down,
    out_weight,
    mixer_out,
    moe_out,
    tokens,
    moe_rows,
    normed_ref,
    rank_ref,
    heads_all,
    returned,
    shared_all,
    spread_high,
    spread_low,
    mix_weight,
    shared_last,
    q_own,
    q_guest,
    held,
    acc,
    row_max,
    guest_acc,
    guest_max,
    guest_out,
    guest_in,
    guest_lse,
    lse_in,
    scores_even,
    scores_odd,
    tops_even,
    tops_odd,
    picks,
    staged,
    arrived,
    gate_up,
    down,
    shared_both,
    hidden_main,
    hidden_tail,
    results,
    load_sem,
    up_send,
    side_send,
    kv_recv,
    guest_send,
    guest_recv,
    chip_send,
    plane_send,
    piece_recv,
    half_recv,
    block_send,
    block_recv,
    rank_send,
    rank_recv,
    shared_send,
    shared_recv,
    hidden_send,
    hidden_recv,
    heads_send,
    heads_recv,
    result_send,
    result_recv,
    stage_sem,
):
    ep_slots, pairs, _, rows, _ = held.shape
    tp_slots = shared_all.shape[0]
    group = min(2, heads)
    experts = expert_gate.shape[0]
    tile = tops_even.shape[0]
    tiles = rows // tile
    scores, tops = (scores_even, scores_odd), (tops_even, tops_odd)
    me = lax.axis_index("ep")
    ep_count = lax.axis_size("ep")
    chips = ep_count // CORES
    chip = me // CORES
    core = me % CORES
    other = 1 - core
    tp_count = lax.axis_size("tp")
    tp_me = lax.axis_index("tp")
    columns = normed_ref.shape[1] // tp_count
    last = chips - 1
    host = chips - 2
    guests = chips > 2

    barrier = pltpu.get_barrier_semaphore()

    def loop(count, body):
        def step(index, carry):
            body(index)
            return carry

        lax.fori_loop(0, count, step, 0)

    def greet(**where):
        pl.semaphore_signal(barrier, inc=1, device_id=where)

    def chip_at(turn):
        found, way, bit = 0, turn + 1, 1
        while bit < chips:
            found = found + ((chip // bit) % 2 + (way // bit) % 2) % 2 * bit
            bit *= 2
        return found

    def tp_at(turn):
        return lax.rem(tp_me + turn + 1, tp_count)

    def ep_at(turn):
        return lax.rem(me + turn + 1, ep_count)

    def lanes_at(index, width):
        return pl.ds(pl.multiple_of(index * width, width), width)

    loads = [
        pltpu.make_async_copy(moe_hbm, moe_rows, load_sem.at[0]),
        pltpu.make_async_copy(q_hbm, q_own, load_sem.at[1]),
    ]
    for pair in range(pairs):
        lanes = pl.ds(pair * LANES, LANES)
        for part, source in enumerate((k_hbm, v_hbm)):
            loads.append(
                pltpu.make_async_copy(
                    source.at[:, lanes],
                    held.at[me, pair, part],
                    load_sem.at[len(loads)],
                )
            )
    weights = []
    for source, place in (
        (shared_gate, shared_both.at[:, pl.ds(0, LANES)]),
        (shared_up, shared_both.at[:, pl.ds(LANES, LANES)]),
        (expert_gate, gate_up.at[:, :, pl.ds(0, LANES)]),
        (expert_up, gate_up.at[:, :, pl.ds(LANES, LANES)]),
        (expert_down, down),
        (shared_down, shared_last),
        (out_weight, mix_weight),
    ):
        index = len(loads) + len(weights)
        weights.append(pltpu.make_async_copy(source, place, load_sem.at[index]))
    for one in loads + weights:
        one.start()

    loop(ep_count - 1, lambda turn: greet(ep=ep_at(turn)))
    loop(tp_count - 1, lambda turn: greet(tp=tp_at(turn)))

    token_count = normed_ref.shape[0]
    slot_rows = arrived.shape[1]
    tail_rows = slot_rows - experts * main
    tail_at = experts * main
    loads[0].wait()
    token = moe_rows[...].astype(jnp.float32)
    square = jnp.mean(token * token, axis=1, keepdims=True)
    token = token * lax.rsqrt(square + norm_eps) * gain_ref[...]
    normed_ref[...] = token.astype(jnp.bfloat16)

    expert_lanes = -(-experts * ep_slots // LANES) * LANES
    top_count = routes_ref.shape[0]
    turned_shape = (expert_lanes, token_count)
    expert_id = lax.broadcasted_iota(jnp.int32, turned_shape, 0)
    named = expert_id == routes_ref[0:1, :]
    for choice in range(1, top_count):
        named = jnp.logical_or(named, expert_id == routes_ref[choice : choice + 1, :])
    named = jnp.where(named, 1.0, 0.0)
    square_shape = (token_count, token_count)
    first_id = lax.broadcasted_iota(jnp.int32, square_shape, 0)
    second_id = lax.broadcasted_iota(jnp.int32, square_shape, 1)
    earlier = jnp.where(first_id < second_id, 1.0, 0.0).astype(jnp.bfloat16)
    turned = jnp.dot(named.astype(jnp.bfloat16), earlier, preferred_element_type=jnp.float32)
    turned = jnp.where(named > 0.0, turned, -1.0)
    for owner in range(ep_slots):
        rank_ref[owner] = turned[owner * experts : (owner + 1) * experts, :]

    def spread_stage():
        owner = jnp.zeros(turned_shape, jnp.int32)
        for index in range(1, ep_slots):
            owner = owner + jnp.where(expert_id >= index * experts, 1, 0)
        local_id = (expert_id - owner * experts).astype(jnp.float32)
        spot = jnp.where(
            turned < main,
            local_id * main + turned,
            local_id * tail + turned + (tail_at - main),
        )
        order = lax.broadcasted_iota(jnp.int32, (ROW_TILE, token_count), 0)
        table = jnp.zeros((ROW_TILE, token_count), jnp.float32)
        for choice in range(top_count):
            hit = expert_id == routes_ref[choice : choice + 1, :]
            place = jnp.sum(jnp.where(hit, spot, 0.0), axis=0, keepdims=True)
            home = jnp.sum(jnp.where(hit, owner, 0).astype(jnp.float32), axis=0, keepdims=True)
            weight = weight_ref[choice : choice + 1, :]
            high = weight.astype(jnp.bfloat16).astype(jnp.float32)
            for part, value in enumerate((place, home, high, weight - high)):
                table = jnp.where(order == part * top_count + choice, value, table)
        same = jnp.where(first_id == second_id, 1.0, 0.0).astype(jnp.bfloat16)
        table = lax.dot_general(
            same,
            table.astype(jnp.bfloat16),
            (((1,), (1,)), ((), ())),
            preferred_element_type=jnp.float32,
        )
        width = ep_slots * slot_rows
        spots = lax.broadcasted_iota(jnp.int32, (token_count, width), 1).astype(jnp.float32)
        high = jnp.zeros((token_count, width), jnp.float32)
        low = jnp.zeros((token_count, width), jnp.float32)

        def column(part, choice):
            index = part * top_count + choice
            return table[:, index : index + 1]

        for choice in range(top_count):
            hit = spots == column(0, choice) + column(1, choice) * slot_rows
            high = jnp.where(hit, column(2, choice), high)
            low = jnp.where(hit, column(3, choice), low)
        spread_high[...] = high.astype(jnp.bfloat16)
        spread_low[...] = low.astype(jnp.bfloat16)

    pl.semaphore_wait(barrier, ep_count + tp_count - 2)

    def remote(source, target, send, recv, **where):
        return pltpu.make_async_remote_copy(
            src_ref=source, dst_ref=target, send_sem=send, recv_sem=recv, device_id=where
        )

    def rank_copy(target, owner):
        return remote(
            rank_ref.at[target], picks.at[owner], rank_send.at[target], rank_recv.at[owner], ep=target
        )

    def up_copy(slot, pair):
        place = held.at[slot, pair]
        return remote(place, place, up_send.at[slot, pair], kv_recv.at[slot, pair], ep=me + CORES)

    def side_copy(slot, pair):
        place = held.at[slot, pair]
        return remote(
            place, place, side_send.at[slot, pair], kv_recv.at[slot, pair], ep=chip * CORES + other
        )

    def guest_query(pair):
        lanes = lanes_at(pair, LANES)
        return remote(
            q_own.at[:, lanes],
            q_guest.at[:, lanes],
            guest_send.at[0, pair],
            guest_recv.at[0, pair],
            ep=me - CORES,
        )

    def guest_result(pair):
        return remote(
            guest_out.at[pair],
            guest_in.at[pair],
            guest_send.at[1, pair],
            guest_recv.at[1, pair],
            ep=me + CORES,
        )

    def guest_stats(pair):
        return remote(
            guest_lse.at[pair],
            lse_in.at[pair],
            guest_send.at[2, pair],
            guest_recv.at[2, pair],
            ep=me + CORES,
        )

    def chip_copy(target):
        return remote(
            normed_ref.at[:, lanes_at(tp_me, columns)],
            tokens.at[me, :, lanes_at(tp_me, columns)],
            chip_send.at[target],
            piece_recv.at[me, tp_me],
            ep=target * CORES + core,
        )

    def plane_copy(slot, piece, target):
        place = tokens.at[slot, :, lanes_at(piece, columns)]
        return remote(
            place, place, plane_send.at[slot, target], piece_recv.at[slot, piece], tp=target
        )

    x_peer = tp_me + 1 - 2 * (tp_me % 2)
    y_peer = tp_me + 2 - 4 * (tp_me // 2 % 2)
    far_peer = x_peer + 2 - 4 * (x_peer // 2 % 2)
    relay = tp_slots == 4 and normed_ref.shape[0] % (2 * ROW_TILE) == 0

    def near_copy(slot, piece, way):
        place = tokens.at[slot, :, lanes_at(piece, columns)]
        return remote(
            place,
            place,
            plane_send.at[slot, way],
            piece_recv.at[slot, piece],
            tp=(x_peer, y_peer)[way],
        )

    def half_copy(slot, piece, part):
        half = normed_ref.shape[0] // 2
        place = tokens.at[slot, pl.ds(part * half, half), lanes_at(piece, columns)]
        return remote(
            place,
            place,
            plane_send.at[slot, 2 + part],
            half_recv.at[slot, part],
            tp=(y_peer, x_peer)[part],
        )

    def block_copy(source, slot):
        return remote(
            source,
            tokens.at[slot],
            block_send.at[slot],
            block_recv.at[slot],
            ep=chip * CORES + other,
        )

    def shared_copy(owner, target):
        place = shared_all.at[owner]
        return remote(place, place, shared_send.at[target], shared_recv.at[owner], tp=target)

    def hidden_copy(owner, part, target):
        place = hidden_tail.at[owner]
        if not (isinstance(part, int) and part == experts):
            place = hidden_main.at[owner, part]
        return remote(
            place, place, hidden_send.at[part, target], hidden_recv.at[part, owner], tp=target
        )

    wide_heads = heads * HEAD % LANES == 0

    def heads_place(owner, pair):
        if wide_heads:
            return heads_all.at[:, lanes_at(owner * pairs + pair, LANES)]
        return heads_all.at[owner]

    def heads_copy(owner, pair, target):
        place = heads_place(owner, pair)
        return remote(
            place, place, heads_send.at[pair, target], heads_recv.at[pair, owner], tp=target
        )

    def result_copy(target, owner):
        return remote(
            results.at[target],
            returned.at[owner],
            result_send.at[target],
            result_recv.at[owner],
            ep=target,
        )

    loop(ep_count - 1, lambda turn: rank_copy(ep_at(turn), me).start())
    loop(chips - 1, lambda turn: chip_copy(chip_at(turn)).start())
    block_copy(normed_ref, me).start()
    picks[me] = rank_ref[me]
    for one in loads[1:]:
        one.wait()

    for pair in range(pairs):

        @pl.when(chip < last)
        def _():
            up_copy(me, pair).start()

        @pl.when(core == 0)
        def _():
            side_copy(me, pair).start()

        if guests:

            @pl.when(chip == last)
            def _():
                guest_query(pair).start()

    units = [(member, index) for member in range(group) for index in range(tiles)]
    lane = lax.broadcasted_iota(jnp.int32, (rows, LANES), 1)
    scale = jnp.asarray(HEAD**-0.5, jnp.bfloat16)

    def attend(pair, slot, queries, sums, maxima, first):
        def score_unit(unit, way):
            member, index = unit
            span = (index + 1) * tile if first else rows
            query = queries[index * tile : (index + 1) * tile, lanes_at(pair, LANES)] * scale
            query = jnp.where(lane[:tile] // HEAD == member, query, jnp.zeros_like(query))
            gates = gate_ref[pl.ds(pair * group + member, 1), lanes_at(slot, rows)]
            result = lax.dot_general(
                query,
                held[slot, pair, 0, :span, :],
                (((1,), (1,)), ((), ())),
                preferred_element_type=jnp.float32,
            )
            result = result - gates[:, :span]
            if first:
                q_pos = index * tile + lax.broadcasted_iota(jnp.int32, result.shape, 0)
                k_pos = lax.broadcasted_iota(jnp.int32, result.shape, 1)
                result = jnp.where(k_pos <= q_pos, result, neg_fill)
            scores[way][:, :span] = result
            top = jnp.max(result, axis=1, keepdims=True)
            tops[way][...] = jnp.broadcast_to(top, (tile, LANES))

        def value_unit(unit, way):
            member, index = unit
            head = pair * group + member
            q_rows = slice(index * tile, (index + 1) * tile)
            span = (index + 1) * tile if first else rows
            new_max = tops[way][...]
            if not first:
                old_max = maxima[head, q_rows, :]
                new_max = jnp.maximum(old_max, new_max)
            wide = jnp.concatenate([new_max] * (span // LANES), axis=1)
            probs = jnp.exp(scores[way][:, :span] - wide).astype(jnp.bfloat16)
            values = held[slot, pair, 1, :span, :]
            values = jnp.where(lane[:span] // HEAD == member, values, jnp.ones_like(values))
            add = jnp.dot(probs, values, preferred_element_type=jnp.float32)
            if not first:
                add = add + sums[head, q_rows, :] * jnp.exp(old_max - new_max)
            sums[head, q_rows, :] = add
            maxima[head, q_rows, :] = new_max

        score_unit(units[0], 0)
        for turn, unit in enumerate(units):
            if turn + 1 < len(units):
                score_unit(units[turn + 1], (turn + 1) % 2)
            value_unit(unit, turn % 2)

    def spread_pieces(turn):
        slot = chip_at(turn) * CORES + core
        plane_copy(slot, tp_me, tp_me).wait_recv()
        if relay:
            for way in range(2):
                near_copy(slot, tp_me, way).start()
        else:
            loop(tp_count - 1, lambda way: plane_copy(slot, tp_me, tp_at(way)).start())

    def relay_pieces(turn):
        slot = chip_at(turn) * CORES + core
        for way, peer in enumerate((x_peer, y_peer)):
            near_copy(slot, peer, way).wait_recv()
            half_copy(slot, peer, way).start()

    def token_stage():
        loop(chips - 1, spread_pieces)
        if relay:
            loop(chips - 1, relay_pieces)

    def share_blocks(turn):
        slot = chip_at(turn) * CORES + core
        if relay:
            for part in range(2):
                half_copy(slot, far_peer, part).wait_recv()
        else:
            loop(tp_count - 1, lambda way: plane_copy(slot, tp_at(way), tp_me).wait_recv())
        block_copy(tokens.at[slot], slot).start()
        gather(slot)

    def shared_stage():
        for one in weights[:2]:
            one.wait()
        both = jnp.dot(normed_ref[...], shared_both[...], preferred_element_type=jnp.float32)
        shared_all[tp_me] = silu_mul(both)
        loop(tp_count - 1, lambda way: shared_copy(tp_me, tp_at(way)).start())

    def gather_block(slot, block):
        ranks = picks[slot]
        parts = []
        if main:
            order = lax.broadcasted_iota(jnp.int32, (main, token_count), 0).astype(jnp.float32)
            for expert in range(experts):
                hit = ranks[expert : expert + 1, :] == order
                parts.append(jnp.where(hit, 1.0, 0.0))
        if tail_rows:
            order = lax.broadcasted_iota(jnp.int32, (tail_rows, token_count), 0)
            found = jnp.zeros((tail_rows, token_count), jnp.float32)
            for expert in range(experts):
                begin = expert * tail
                wanted = (order - begin + main).astype(jnp.float32)
                hit = ranks[expert : expert + 1, :] == wanted
                inside = jnp.logical_and(order >= begin, order < begin + tail)
                found = jnp.where(jnp.logical_and(hit, inside), 1.0, found)
            parts.append(found)
        pick = jnp.concatenate(parts, axis=0).astype(jnp.bfloat16)
        rows_in = jnp.dot(pick, block, preferred_element_type=jnp.float32)
        arrived[slot] = rows_in.astype(jnp.bfloat16)

    def tail_select(value_of, width):
        order = lax.broadcasted_iota(jnp.int32, (ep_slots, tail_rows, width), 1)
        order = order.reshape(ep_slots * tail_rows, width)
        total = value_of(0)
        for expert in range(1, experts):
            total = jnp.where(order >= expert * tail, value_of(expert), total)
        return total

    def gather(slot):
        if staged is None:
            gather_block(slot, tokens[slot])
        else:
            fetch = pltpu.make_async_copy(tokens.at[slot], staged, stage_sem.at[0])
            fetch.start()
            fetch.wait()
            gather_block(slot, staged[...])

    def share_stage():
        loop(ep_count - 1, lambda turn: rank_copy(ep_at(turn), ep_at(turn)).wait_recv())
        gather_block(me, normed_ref[...])
        loop(chips - 1, share_blocks)

    def up_stage():
        def finish_block(index):
            slot = index * CORES + other
            block_copy(tokens.at[slot], slot).wait_recv()
            gather(slot)

        finish_block(chip)
        loop(chips - 1, lambda turn: finish_block(chip_at(turn)))
        for one in weights[2:4]:
            one.wait()
        depth = arrived.shape[2]
        if tail_rows:
            block = arrived[:, tail_at:, :].reshape(ep_slots * tail_rows, depth)
            both = tail_select(
                lambda e: jnp.dot(block, gate_up[e], preferred_element_type=jnp.float32),
                2 * LANES,
            )
            hidden_tail[tp_me] = silu_mul(both)
            loop(tp_count - 1, lambda way: hidden_copy(tp_me, experts, tp_at(way)).start())
        if main:

            def expert_step(expert):
                span = pl.ds(pl.multiple_of(expert * main, main), main)
                block = arrived[:, span, :].reshape(ep_slots * main, depth)
                both = jnp.dot(block, gate_up[expert], preferred_element_type=jnp.float32)
                hidden_main[tp_me, expert] = silu_mul(both)
                loop(tp_count - 1, lambda way: hidden_copy(tp_me, expert, tp_at(way)).start())

            loop(experts, expert_step)

    def down_stage():
        weights[4].wait()
        width = down.shape[2]

        def arrival(part):
            loop(tp_count - 1, lambda way: hidden_copy(tp_at(way), part, tp_me).wait_recv())

        if tail_rows:
            arrival(experts)
            block = jnp.concatenate([hidden_tail[piece] for piece in range(tp_slots)], axis=1)
            out = tail_select(
                lambda e: jnp.dot(block, down[e], preferred_element_type=jnp.float32), width
            )
            out = out.astype(jnp.bfloat16).reshape(ep_slots, tail_rows, width)
            results[:, tail_at:, :] = out
        if main:

            def expert_step(expert):
                arrival(expert)
                span = pl.ds(pl.multiple_of(expert * main, main), main)
                pieces = [hidden_main[piece, expert] for piece in range(tp_slots)]
                block = jnp.concatenate(pieces, axis=1)
                out = jnp.dot(block, down[expert], preferred_element_type=jnp.float32)
                results[:, span, :] = out.astype(jnp.bfloat16).reshape(ep_slots, main, width)

            loop(experts, expert_step)
        loop(ep_count - 1, lambda turn: result_copy(ep_at(turn), me).start())
        returned[me] = results[me]

    def ratio(sums, head):
        whole = sums[head]
        return whole / pltpu.roll(whole, HEAD, 1)

    def pair_out(sums, pair):
        joined = ratio(sums, pair * group)
        if group == 1:
            joined = jnp.where(lane < HEAD, joined, 0.0)
        else:
            joined = jnp.where(lane < HEAD, joined, ratio(sums, pair * group + 1))
        return joined.astype(jnp.bfloat16)

    def send_guest(pair):
        guest_out[pair] = pair_out(guest_acc, pair)
        stats = jnp.zeros((rows, LANES), jnp.float32)
        for member in range(group):
            whole = guest_acc[pair * group + member]
            total = jnp.where(lane // HEAD == member, pltpu.roll(whole, HEAD, 1), whole)
            value = guest_max[pair * group + member] + jnp.log(total)
            stats = jnp.where(lane == member, value, stats)
        guest_lse[pair] = stats.T[:8, :]
        guest_result(pair).start()
        guest_stats(pair).start()

    def merge_guest(pair):
        guest_result(pair).wait_recv()
        guest_stats(pair).wait_recv()
        stats = jnp.concatenate([lse_in[pair]] * (LANES // 8), axis=0).T
        outer = guest_in[pair].astype(jnp.float32)
        for member in range(group):
            head = pair * group + member
            value = jnp.broadcast_to(stats[:, member : member + 1], (rows, LANES))
            new_max = jnp.maximum(row_max[head], value)
            part = jnp.where(lane // HEAD == member, outer, 1.0)
            acc[head] = acc[head] * jnp.exp(row_max[head] - new_max) + part * jnp.exp(
                value - new_max
            )

    def finish_pair(pair):
        if guests:

            @pl.when(chip == last)
            def _():
                merge_guest(pair)

        if wide_heads:
            heads_all[:, lanes_at(tp_me * pairs + pair, LANES)] = pair_out(acc, pair)
        else:
            heads_all[tp_me] = pair_out(acc, pair)
        loop(tp_count - 1, lambda way: heads_copy(tp_me, pair, tp_at(way)).start())

    reach = 1 if guests else chips
    deepest = jnp.where(chip == last, jnp.minimum(chip, reach), chip)
    step_count = deepest * CORES + core
    steps = max(CORES * (host if guests else last) + 1, CORES + 1)
    delay = 3 if guests else 1
    total = pairs * (steps + 1)

    def remote_step(pair, step):
        turn = step - core + CORES
        own_core = turn % CORES == 0
        back = turn // CORES
        slot = (chip - back) * CORES + jnp.where(own_core, core, other)
        side_copy(slot, pair).wait_recv()

        @pl.when(jnp.logical_and(own_core, chip < (host if guests else last)))
        def _():
            up_copy(slot, pair).start()

        @pl.when(own_core)
        def _():
            side_copy(slot, pair).start()

        attend(pair, slot, q_own, acc, row_max, False)
        if guests:

            @pl.when(jnp.logical_and(chip == host, back >= 1))
            def _():
                @pl.when(step == core)
                def _():
                    guest_query(pair).wait_recv()
                    for member in range(group):
                        head = pair * group + member
                        guest_acc[head] = jnp.zeros((rows, LANES), jnp.float32)
                        guest_max[head] = jnp.full((rows, LANES), neg_fill, jnp.float32)

                attend(pair, slot, q_guest, guest_acc, guest_max, False)

    hooks = (
        (1, shared_stage),
        (1, spread_stage),
        (pairs, token_stage),
        (pairs + 1, share_stage),
        (pairs + 2, up_stage),
        (total, down_stage),
    )

    def one_turn(index):
        for at, stage in hooks:
            pl.when(index == at)(stage)

        @pl.when(index < pairs)
        def _():
            attend(index, me, q_own, acc, row_max, True)

        @pl.when(jnp.logical_and(index >= pairs, index < total))
        def _():
            pair = (index - pairs) // steps
            step = (index - pairs) % steps

            @pl.when(step < step_count)
            def _():
                remote_step(pair, step)

            if guests:

                @pl.when(jnp.logical_and(chip == host, step == steps - 1))
                def _():
                    send_guest(pair)

        late = index - pairs - jnp.where(chip == last, delay, 0)

        @pl.when(jnp.logical_and(late >= 0, late < pairs * steps))
        def _():
            @pl.when(late % steps == steps - 1)
            def _():
                finish_pair(late // steps)

    loop(total + delay, one_turn)

    for pair in range(pairs):

        def finish_kv(back):
            slot = (chip - back) * CORES + core

            @pl.when(
                jnp.logical_or(
                    chip < (host if guests else last), jnp.logical_and(back == 0, chip < last)
                )
            )
            def _():
                up_copy(slot, pair).wait_send()

            @pl.when(back > 0)
            def _():
                side_copy(slot, pair).wait_send()

        loop(deepest + 1, finish_kv)

        @pl.when(core == 0)
        def _():
            side_copy(me, pair).wait_send()

        if guests:

            @pl.when(chip == last)
            def _():
                guest_query(pair).wait_send()

            @pl.when(chip == host)
            def _():
                guest_result(pair).wait_send()
                guest_stats(pair).wait_send()

    def finish_tokens(turn):
        target = chip_at(turn)
        slot = target * CORES + core
        chip_copy(target).wait_send()
        if relay:
            for way, peer in enumerate((x_peer, y_peer)):
                near_copy(slot, tp_me, way).wait_send()
                half_copy(slot, peer, way).wait_send()
        else:
            loop(tp_count - 1, lambda way: plane_copy(slot, tp_me, tp_at(way)).wait_send())
        block_copy(tokens.at[slot], slot).wait_send()

    loop(chips - 1, finish_tokens)
    block_copy(normed_ref, me).wait_send()

    def finish_peers(turn):
        rank_copy(ep_at(turn), me).wait_send()
        result_copy(ep_at(turn), me).wait_send()
        result_copy(ep_at(turn), ep_at(turn)).wait_recv()

    loop(ep_count - 1, finish_peers)

    def finish_plane(way):
        peer = tp_at(way)
        shared_copy(tp_me, peer).wait_send()
        shared_copy(peer, peer).wait_recv()
        for part in range(experts + 1):
            if tail_rows if part == experts else main:
                hidden_copy(tp_me, part, peer).wait_send()
        for pair in range(pairs):
            heads_copy(tp_me, pair, peer).wait_send()
            heads_copy(peer, pair, peer).wait_recv()

    loop(tp_count - 1, finish_plane)
    for one in weights[5:]:
        one.wait()
    shared_hidden = jnp.concatenate([shared_all[piece] for piece in range(tp_slots)], axis=1)
    back = returned[...].reshape(ep_slots * slot_rows, returned.shape[2])
    sums = jnp.dot(shared_hidden, shared_last[...], preferred_element_type=jnp.float32)
    for part in (spread_high, spread_low):
        sums = sums + jnp.dot(part[...], back, preferred_element_type=jnp.float32)
    moe_out[...] = sums.astype(jnp.bfloat16)
    if wide_heads:
        mixed = heads_all[...]
    else:
        mixed = jnp.concatenate([heads_all[piece] for piece in range(tp_slots)], axis=1)
    mixed = jnp.dot(mixed, mix_weight[...], preferred_element_type=jnp.float32)
    mixer_out[...] = mixed.astype(jnp.bfloat16)


def slot_layout(capacity, experts):
    main = capacity // ROW_TILE * ROW_TILE
    tail = capacity - main
    tail_rows = -(-tail * experts // ROW_TILE) * ROW_TILE
    return main, tail, experts * main + tail_rows


def padded(a, axis, to):
    if a.shape[axis] == to:
        return a
    spare = [(0, 0)] * a.ndim
    spare[axis] = (0, to - a.shape[axis])
    return jnp.pad(a, spare)


def fused_block(
    query_rows,
    key_rows,
    value_rows,
    cum_gate,
    routes,
    route_weight,
    moe_gain,
    moe_input,
    expert_gate,
    expert_up,
    expert_down,
    shared_gate,
    shared_up,
    shared_down,
    out_weight,
):
    rows, width = query_rows.shape
    heads = width // HEAD
    pairs = (heads + 1) // 2
    ep_count = lax.axis_size("ep")
    tp_count = lax.axis_size("tp")
    chips = ep_count // CORES
    lanes = pairs * LANES
    tile = rows // 2 if rows % (2 * LANES) == 0 else rows
    query_rows, key_rows, value_rows = (
        padded(a, 1, lanes) for a in (query_rows, key_rows, value_rows)
    )
    experts, depth, span = expert_gate.shape
    columns = expert_down.shape[2]
    token_count = moe_input.shape[0]
    capacity = 2 * token_count * routes.shape[1] // (experts * ep_count)
    main, tail, slot_rows = slot_layout(capacity, experts)
    if span < LANES:
        expert_gate, expert_up = padded(expert_gate, 2, LANES), padded(expert_up, 2, LANES)
        shared_gate, shared_up = padded(shared_gate, 1, LANES), padded(shared_up, 1, LANES)
        expert_down = padded(expert_down.reshape(experts, tp_count, span, columns), 2, LANES)
        expert_down = expert_down.reshape(experts, tp_count * LANES, columns)
        shared_down = padded(shared_down.reshape(tp_count, span, columns), 1, LANES)
        shared_down = shared_down.reshape(tp_count * LANES, columns)
    inside = ep_count * token_count * depth * 2 <= 8 * 1024 * 1024
    bf16, f32 = jnp.bfloat16, jnp.float32
    vmem = pl.BlockSpec(memory_space=pltpu.VMEM)
    anywhere = pl.BlockSpec(memory_space=pl.ANY)
    if width % LANES:
        out_weight = padded(out_weight.reshape(tp_count, width, columns), 1, LANES)
        out_weight = out_weight.reshape(tp_count * LANES, columns)
    heads_shape = (rows, tp_count * width) if width % LANES == 0 else (tp_count, rows, LANES)
    outs = [
        jax.ShapeDtypeStruct((rows, columns), bf16),
        jax.ShapeDtypeStruct((token_count, columns), bf16),
    ]
    out_specs = [vmem] * 2
    token_shape = (ep_count, token_count, depth)
    scratch = []
    if inside:
        scratch.append(pltpu.VMEM(token_shape, bf16))
    else:
        outs.append(jax.ShapeDtypeStruct(token_shape, bf16))
        out_specs.append(anywhere)
    dma = pltpu.SemaphoreType.DMA
    scratch += [
        pltpu.VMEM((token_count, depth), bf16),
        pltpu.VMEM((token_count, depth), bf16),
        pltpu.VMEM((ep_count, experts, token_count), f32),
        pltpu.VMEM(heads_shape, bf16),
        pltpu.VMEM((ep_count, slot_rows, columns), bf16),
        pltpu.VMEM((tp_count, token_count, LANES), bf16),
        pltpu.VMEM((token_count, ep_count * slot_rows), bf16),
        pltpu.VMEM((token_count, ep_count * slot_rows), bf16),
        pltpu.VMEM(out_weight.shape, bf16),
        pltpu.VMEM(shared_down.shape, bf16),
        pltpu.VMEM((rows, lanes), bf16),
        pltpu.VMEM((rows, lanes), bf16),
        pltpu.VMEM((ep_count, pairs, 2, rows, LANES), bf16),
        pltpu.VMEM((heads, rows, LANES), f32),
        pltpu.VMEM((heads, rows, LANES), f32),
        pltpu.VMEM((heads, rows, LANES), f32),
        pltpu.VMEM((heads, rows, LANES), f32),
        pltpu.VMEM((pairs, rows, LANES), bf16),
        pltpu.VMEM((pairs, rows, LANES), bf16),
        pltpu.VMEM((pairs, 8, rows), f32),
        pltpu.VMEM((pairs, 8, rows), f32),
        pltpu.VMEM((tile, rows), f32),
        pltpu.VMEM((tile, rows), f32),
        pltpu.VMEM((tile, LANES), f32),
        pltpu.VMEM((tile, LANES), f32),
        pltpu.VMEM((ep_count, experts, token_count), f32),
    ]
    if not inside:
        scratch.append(pltpu.VMEM((token_count, depth), bf16))
    scratch += [
        pltpu.VMEM((ep_count, slot_rows, depth), bf16),
        pltpu.VMEM((experts, depth, 2 * LANES), bf16),
        pltpu.VMEM(expert_down.shape, bf16),
        pltpu.VMEM((depth, 2 * LANES), bf16),
        pltpu.VMEM((tp_count, experts, ep_count * max(main, 1), LANES), bf16),
        pltpu.VMEM((tp_count, max(ep_count * (slot_rows - experts * main), 8), LANES), bf16),
        pltpu.VMEM((ep_count, slot_rows, columns), bf16),
        dma((9 + 2 * pairs,)),
        dma((ep_count, pairs)),
        dma((ep_count, pairs)),
        dma((ep_count, pairs)),
        dma((3, pairs)),
        dma((3, pairs)),
        dma((chips,)),
        dma((ep_count, tp_count)),
        dma((ep_count, tp_count)),
        dma((ep_count, 2)),
        dma((ep_count,)),
        dma((ep_count,)),
        dma((ep_count,)),
        dma((ep_count,)),
        dma((tp_count,)),
        dma((tp_count,)),
        dma((experts + 1, tp_count)),
        dma((experts + 1, tp_count)),
        dma((pairs, tp_count)),
        dma((pairs, tp_count)),
        dma((ep_count,)),
        dma((ep_count,)),
        dma((2,)),
    ]
    body = functools.partial(block_kernel, heads, main, tail)
    inputs = 15

    def kernel(*refs):
        refs = list(refs)
        if inside:
            refs.insert(inputs + 2 + 27, None)
        body(*refs)

    blocks = ep_count * rows * rows * heads
    return pl.pallas_call(
        kernel,
        out_shape=outs,
        in_specs=[anywhere] * 3 + [vmem] * 4 + [anywhere] * 8,
        out_specs=out_specs,
        scratch_shapes=scratch,
        compiler_params=pltpu.CompilerParams(
            collective_id=0, has_side_effects=True, vmem_limit_bytes=58 * 1024 * 1024
        ),
        cost_estimate=pl.CostEstimate(
            flops=blocks * 2 * 512, bytes_accessed=8 * 1024 * 1024, transcendentals=blocks
        ),
        name="fused_block",
    )(
        query_rows,
        key_rows,
        value_rows,
        cum_gate,
        routes.T,
        route_weight.T,
        moe_gain[None, :],
        moe_input,
        expert_gate,
        expert_up,
        expert_down,
        shared_gate,
        shared_up,
        shared_down,
        out_weight,
    )[:2]


def local(
    query_rows,
    key_rows,
    value_rows,
    cum_gate,
    out_weight,
    moe_input,
    moe_gain,
    routes,
    route_weight,
    expert_gate,
    expert_up,
    expert_down,
    shared_gate,
    shared_up,
    shared_down,
):
    mixer, moe = fused_block(
        query_rows,
        key_rows,
        value_rows,
        cum_gate,
        routes,
        route_weight,
        moe_gain,
        moe_input,
        expert_gate,
        expert_up,
        expert_down,
        shared_gate,
        shared_up,
        shared_down,
        out_weight,
    )
    return (mixer, moe)


def solution(mesh):
    placed = (
        P("ep", "tp"),
        P("ep", "tp"),
        P("ep", "tp"),
        P("tp", None),
        P(None, "tp"),
        P("ep", None),
        P(),
        P("ep", None),
        P("ep", None),
        P("ep", None, "tp"),
        P("ep", None, "tp"),
        P("ep", None, "tp"),
        P(None, "tp"),
        P(None, "tp"),
        P(None, "tp"),
    )
    return jax.shard_map(
        local, mesh=mesh, in_specs=placed, out_specs=(P("ep", "tp"), P("ep", "tp")), check_vma=False
    )
```

```python
import functools

import jax
import jax.numpy as jnp
from jax import lax
from jax.experimental import pallas as pl
from jax.experimental.pallas import tpu as pltpu
from jax.sharding import PartitionSpec as P

HEAD = 64
LANES = 128
CORES = 2
ROW_TILE = 16

neg_fill = -1e30
norm_eps = 1e-06


def silu_mul(both):
    gate, up = both[:, :LANES], both[:, LANES:]
    return (gate / (1.0 + jnp.exp(-gate)) * up).astype(jnp.bfloat16)


def block_kernel(
    heads,
    main,
    tail,
    q_hbm,
    k_hbm,
    v_hbm,
    gate_ref,
    routes_ref,
    weight_ref,
    gain_ref,
    moe_hbm,
    expert_gate,
    expert_up,
    expert_down,
    shared_gate,
    shared_up,
    shared_down,
    out_weight,
    mixer_out,
    moe_out,
    tokens,
    moe_rows,
    normed_ref,
    rank_ref,
    heads_all,
    returned,
    shared_all,
    spread_high,
    spread_low,
    mix_weight,
    shared_last,
    q_own,
    q_guest,
    held,
    acc,
    row_max,
    guest_acc,
    guest_max,
    guest_out,
    guest_in,
    guest_lse,
    lse_in,
    scores_even,
    scores_odd,
    tops_even,
    tops_odd,
    picks,
    staged,
    arrived,
    gate_up,
    down,
    shared_both,
    hidden_main,
    hidden_tail,
    results,
    load_sem,
    up_send,
    side_send,
    kv_recv,
    guest_send,
    guest_recv,
    chip_send,
    plane_send,
    piece_recv,
    half_recv,
    block_send,
    block_recv,
    rank_send,
    rank_recv,
    shared_send,
    shared_recv,
    hidden_send,
    hidden_recv,
    heads_send,
    heads_recv,
    result_send,
    result_recv,
    stage_sem,
):
    ep_slots, pairs, _, rows, _ = held.shape
    tp_slots = shared_all.shape[0]
    group = min(2, heads)
    experts = expert_gate.shape[0]
    tile = tops_even.shape[0]
    tiles = rows // tile
    scores, tops = (scores_even, scores_odd), (tops_even, tops_odd)
    me = lax.axis_index("ep")
    ep_count = lax.axis_size("ep")
    chips = ep_count // CORES
    chip = me // CORES
    core = me % CORES
    other = 1 - core
    tp_count = lax.axis_size("tp")
    tp_me = lax.axis_index("tp")
    columns = normed_ref.shape[1] // tp_count
    last = chips - 1
    host = chips - 3
    limit = chips - 2
    hops = 2 * CORES
    guests = chips > 2

    barrier = pltpu.get_barrier_semaphore()

    def loop(count, body):
        def step(index, carry):
            body(index)
            return carry

        lax.fori_loop(0, count, step, 0)

    def greet(**where):
        pl.semaphore_signal(barrier, inc=1, device_id=where)

    def chip_at(turn):
        found, way, bit = 0, turn + 1, 1
        while bit < chips:
            found = found + ((chip // bit) % 2 + (way // bit) % 2) % 2 * bit
            bit *= 2
        return found

    def tp_at(turn):
        return lax.rem(tp_me + turn + 1, tp_count)

    def ep_at(turn):
        return lax.rem(me + turn + 1, ep_count)

    def lanes_at(index, width):
        return pl.ds(pl.multiple_of(index * width, width), width)

    loads = [
        pltpu.make_async_copy(moe_hbm, moe_rows, load_sem.at[0]),
        pltpu.make_async_copy(q_hbm, q_own, load_sem.at[1]),
    ]
    for pair in range(pairs):
        lanes = pl.ds(pair * LANES, LANES)
        for part, source in enumerate((k_hbm, v_hbm)):
            loads.append(
                pltpu.make_async_copy(
                    source.at[:, lanes],
                    held.at[me, pair, part],
                    load_sem.at[len(loads)],
                )
            )
    weights = []
    for source, place in (
        (shared_gate, shared_both.at[:, pl.ds(0, LANES)]),
        (shared_up, shared_both.at[:, pl.ds(LANES, LANES)]),
        (expert_gate, gate_up.at[:, :, pl.ds(0, LANES)]),
        (expert_up, gate_up.at[:, :, pl.ds(LANES, LANES)]),
        (expert_down, down),
        (shared_down, shared_last),
        (out_weight, mix_weight),
    ):
        index = len(loads) + len(weights)
        weights.append(pltpu.make_async_copy(source, place, load_sem.at[index]))
    for one in loads + weights:
        one.start()

    loop(ep_count - 1, lambda turn: greet(ep=ep_at(turn)))
    loop(tp_count - 1, lambda turn: greet(tp=tp_at(turn)))

    token_count = normed_ref.shape[0]
    slot_rows = arrived.shape[1]
    tail_rows = slot_rows - experts * main
    tail_at = experts * main
    loads[0].wait()
    token = moe_rows[...].astype(jnp.float32)
    square = jnp.mean(token * token, axis=1, keepdims=True)
    token = token * lax.rsqrt(square + norm_eps) * gain_ref[...]
    normed_ref[...] = token.astype(jnp.bfloat16)

    expert_lanes = -(-experts * ep_slots // LANES) * LANES
    top_count = routes_ref.shape[0]
    turned_shape = (expert_lanes, token_count)
    expert_id = lax.broadcasted_iota(jnp.int32, turned_shape, 0)
    named = expert_id == routes_ref[0:1, :]
    for choice in range(1, top_count):
        named = jnp.logical_or(named, expert_id == routes_ref[choice : choice + 1, :])
    named = jnp.where(named, 1.0, 0.0)
    square_shape = (token_count, token_count)
    first_id = lax.broadcasted_iota(jnp.int32, square_shape, 0)
    second_id = lax.broadcasted_iota(jnp.int32, square_shape, 1)
    earlier = jnp.where(first_id < second_id, 1.0, 0.0).astype(jnp.bfloat16)
    turned = jnp.dot(named.astype(jnp.bfloat16), earlier, preferred_element_type=jnp.float32)
    turned = jnp.where(named > 0.0, turned, -1.0)
    for owner in range(ep_slots):
        rank_ref[owner] = turned[owner * experts : (owner + 1) * experts, :]

    def spread_stage():
        owner = jnp.zeros(turned_shape, jnp.int32)
        for index in range(1, ep_slots):
            owner = owner + jnp.where(expert_id >= index * experts, 1, 0)
        local_id = (expert_id - owner * experts).astype(jnp.float32)
        spot = jnp.where(
            turned < main,
            local_id * main + turned,
            local_id * tail + turned + (tail_at - main),
        )
        order = lax.broadcasted_iota(jnp.int32, (ROW_TILE, token_count), 0)
        table = jnp.zeros((ROW_TILE, token_count), jnp.float32)
        for choice in range(top_count):
            hit = expert_id == routes_ref[choice : choice + 1, :]
            place = jnp.sum(jnp.where(hit, spot, 0.0), axis=0, keepdims=True)
            home = jnp.sum(jnp.where(hit, owner, 0).astype(jnp.float32), axis=0, keepdims=True)
            weight = weight_ref[choice : choice + 1, :]
            high = weight.astype(jnp.bfloat16).astype(jnp.float32)
            for part, value in enumerate((place, home, high, weight - high)):
                table = jnp.where(order == part * top_count + choice, value, table)
        same = jnp.where(first_id == second_id, 1.0, 0.0).astype(jnp.bfloat16)
        table = lax.dot_general(
            same,
            table.astype(jnp.bfloat16),
            (((1,), (1,)), ((), ())),
            preferred_element_type=jnp.float32,
        )
        width = ep_slots * slot_rows
        spots = lax.broadcasted_iota(jnp.int32, (token_count, width), 1).astype(jnp.float32)
        high = jnp.zeros((token_count, width), jnp.float32)
        low = jnp.zeros((token_count, width), jnp.float32)

        def column(part, choice):
            index = part * top_count + choice
            return table[:, index : index + 1]

        for choice in range(top_count):
            hit = spots == column(0, choice) + column(1, choice) * slot_rows
            high = jnp.where(hit, column(2, choice), high)
            low = jnp.where(hit, column(3, choice), low)
        spread_high[...] = high.astype(jnp.bfloat16)
        spread_low[...] = low.astype(jnp.bfloat16)

    pl.semaphore_wait(barrier, ep_count + tp_count - 2)

    def remote(source, target, send, recv, **where):
        return pltpu.make_async_remote_copy(
            src_ref=source, dst_ref=target, send_sem=send, recv_sem=recv, device_id=where
        )

    def rank_copy(target, owner):
        return remote(
            rank_ref.at[target], picks.at[owner], rank_send.at[target], rank_recv.at[owner], ep=target
        )

    def up_copy(slot, pair):
        place = held.at[slot, pair]
        return remote(place, place, up_send.at[slot, pair], kv_recv.at[slot, pair], ep=me + CORES)

    def side_copy(slot, pair):
        place = held.at[slot, pair]
        return remote(
            place, place, side_send.at[slot, pair], kv_recv.at[slot, pair], ep=chip * CORES + other
        )

    def guest_query(pair):
        lanes = lanes_at(pair, LANES)
        return remote(
            q_own.at[:, lanes],
            q_guest.at[:, lanes],
            guest_send.at[0, pair],
            guest_recv.at[0, pair],
            ep=me - hops,
        )

    def guest_result(pair):
        return remote(
            guest_out.at[pair],
            guest_in.at[pair],
            guest_send.at[1, pair],
            guest_recv.at[1, pair],
            ep=me + hops,
        )

    def guest_stats(pair):
        return remote(
            guest_lse.at[pair],
            lse_in.at[pair],
            guest_send.at[2, pair],
            guest_recv.at[2, pair],
            ep=me + hops,
        )

    def hop_copy(slot, way, source=None):
        place = tokens.at[slot, :, lanes_at(tp_me, columns)]
        return remote(
            place if source is None else source,
            place,
            chip_send.at[slot, way],
            piece_recv.at[slot, tp_me],
            ep=me + (CORES, -CORES)[way],
        )

    def own_hop(way):
        return hop_copy(me, way, normed_ref.at[:, lanes_at(tp_me, columns)])

    def plane_copy(slot, piece, target):
        place = tokens.at[slot, :, lanes_at(piece, columns)]
        return remote(
            place, place, plane_send.at[slot, target], piece_recv.at[slot, piece], tp=target
        )

    x_peer = tp_me + 1 - 2 * (tp_me % 2)
    y_peer = tp_me + 2 - 4 * (tp_me // 2 % 2)
    far_peer = x_peer + 2 - 4 * (x_peer // 2 % 2)
    relay = tp_slots == 4 and normed_ref.shape[0] % (2 * ROW_TILE) == 0

    def near_copy(slot, piece, way):
        place = tokens.at[slot, :, lanes_at(piece, columns)]
        return remote(
            place,
            place,
            plane_send.at[slot, way],
            piece_recv.at[slot, piece],
            tp=(x_peer, y_peer)[way],
        )

    def half_copy(slot, piece, part):
        half = normed_ref.shape[0] // 2
        place = tokens.at[slot, pl.ds(part * half, half), lanes_at(piece, columns)]
        return remote(
            place,
            place,
            plane_send.at[slot, 2 + part],
            half_recv.at[slot, part],
            tp=(y_peer, x_peer)[part],
        )

    def block_copy(source, slot):
        return remote(
            source,
            tokens.at[slot],
            block_send.at[slot],
            block_recv.at[slot],
            ep=chip * CORES + other,
        )

    def shared_copy(owner, target):
        place = shared_all.at[owner]
        return remote(place, place, shared_send.at[target], shared_recv.at[owner], tp=target)

    def hidden_copy(owner, part, target):
        place = hidden_tail.at[owner]
        if not (isinstance(part, int) and part == experts):
            place = hidden_main.at[owner, part]
        return remote(
            place, place, hidden_send.at[part, target], hidden_recv.at[part, owner], tp=target
        )

    wide_heads = heads * HEAD % LANES == 0

    def heads_place(owner, pair):
        if wide_heads:
            return heads_all.at[:, lanes_at(owner * pairs + pair, LANES)]
        return heads_all.at[owner]

    def heads_copy(owner, pair, target):
        place = heads_place(owner, pair)
        return remote(
            place, place, heads_send.at[pair, target], heads_recv.at[pair, owner], tp=target
        )

    def result_copy(target, owner):
        return remote(
            results.at[target],
            returned.at[owner],
            result_send.at[target],
            result_recv.at[owner],
            ep=target,
        )

    loop(ep_count - 1, lambda turn: rank_copy(ep_at(turn), me).start())
    higher, lower = chip < last, chip > 0
    pl.when(higher)(lambda: own_hop(0).start())
    pl.when(lower)(lambda: own_hop(1).start())
    block_copy(normed_ref, me).start()
    picks[me] = rank_ref[me]
    for one in loads[1:]:
        one.wait()

    paired = jnp.logical_and(chip == host, guests)

    for pair in range(pairs):

        @pl.when(chip < last)
        def _():
            up_copy(me, pair).start()

        @pl.when(jnp.logical_or(core == 0, paired))
        def _():
            side_copy(me, pair).start()

        if guests:

            @pl.when(chip == last)
            def _():
                guest_query(pair).start()

    units = [(member, index) for member in range(group) for index in range(tiles)]
    lane = lax.broadcasted_iota(jnp.int32, (rows, LANES), 1)
    scale = jnp.asarray(HEAD**-0.5, jnp.bfloat16)

    def attend(pair, slot, queries, sums, maxima, first):
        def score_unit(unit, way):
            member, index = unit
            span = (index + 1) * tile if first else rows
            query = queries[index * tile : (index + 1) * tile, lanes_at(pair, LANES)] * scale
            query = jnp.where(lane[:tile] // HEAD == member, query, jnp.zeros_like(query))
            gates = gate_ref[pl.ds(pair * group + member, 1), lanes_at(slot, rows)]
            result = lax.dot_general(
                query,
                held[slot, pair, 0, :span, :],
                (((1,), (1,)), ((), ())),
                preferred_element_type=jnp.float32,
            )
            result = result - gates[:, :span]
            if first:
                q_pos = index * tile + lax.broadcasted_iota(jnp.int32, result.shape, 0)
                k_pos = lax.broadcasted_iota(jnp.int32, result.shape, 1)
                result = jnp.where(k_pos <= q_pos, result, neg_fill)
            scores[way][:, :span] = result
            top = jnp.max(result, axis=1, keepdims=True)
            tops[way][...] = jnp.broadcast_to(top, (tile, LANES))

        def value_unit(unit, way):
            member, index = unit
            head = pair * group + member
            q_rows = slice(index * tile, (index + 1) * tile)
            span = (index + 1) * tile if first else rows
            new_max = tops[way][...]
            if not first:
                old_max = maxima[head, q_rows, :]
                new_max = jnp.maximum(old_max, new_max)
            wide = jnp.concatenate([new_max] * (span // LANES), axis=1)
            probs = jnp.exp(scores[way][:, :span] - wide).astype(jnp.bfloat16)
            values = held[slot, pair, 1, :span, :]
            values = jnp.where(lane[:span] // HEAD == member, values, jnp.ones_like(values))
            add = jnp.dot(probs, values, preferred_element_type=jnp.float32)
            if not first:
                add = add + sums[head, q_rows, :] * jnp.exp(old_max - new_max)
            sums[head, q_rows, :] = add
            maxima[head, q_rows, :] = new_max

        score_unit(units[0], 0)
        for turn, unit in enumerate(units):
            if turn + 1 < len(units):
                score_unit(units[turn + 1], (turn + 1) % 2)
            value_unit(unit, turn % 2)

    def spread_pieces(slot, way, onward):
        hop_copy(slot, way).wait_recv()
        pl.when(onward)(lambda: hop_copy(slot, way).start())
        if relay:
            for near in range(2):
                near_copy(slot, tp_me, near).start()
        else:
            loop(tp_count - 1, lambda peer: plane_copy(slot, tp_me, tp_at(peer)).start())

    def spread_distance(turn):
        down_slot, up_slot = me - (turn + 1) * CORES, me + (turn + 1) * CORES
        pl.when(down_slot >= 0)(lambda: spread_pieces(down_slot, 0, higher))
        pl.when(up_slot < ep_count)(lambda: spread_pieces(up_slot, 1, lower))

    def relay_pieces(turn):
        slot = chip_at(turn) * CORES + core
        for way, peer in enumerate((x_peer, y_peer)):
            near_copy(slot, peer, way).wait_recv()
            half_copy(slot, peer, way).start()

    def token_stage():
        loop(chips - 1, spread_distance)
        if relay:
            loop(chips - 1, relay_pieces)

    def share_blocks(turn):
        slot = chip_at(turn) * CORES + core
        if relay:
            for part in range(2):
                half_copy(slot, far_peer, part).wait_recv()
        else:
            loop(tp_count - 1, lambda way: plane_copy(slot, tp_at(way), tp_me).wait_recv())
        block_copy(tokens.at[slot], slot).start()
        gather(slot)

    def shared_stage():
        for one in weights[:2]:
            one.wait()
        both = jnp.dot(normed_ref[...], shared_both[...], preferred_element_type=jnp.float32)
        shared_all[tp_me] = silu_mul(both)
        loop(tp_count - 1, lambda way: shared_copy(tp_me, tp_at(way)).start())

    def gather_block(slot, block):
        ranks = picks[slot]
        parts = []
        if main:
            order = lax.broadcasted_iota(jnp.int32, (main, token_count), 0).astype(jnp.float32)
            for expert in range(experts):
                hit = ranks[expert : expert + 1, :] == order
                parts.append(jnp.where(hit, 1.0, 0.0))
        if tail_rows:
            order = lax.broadcasted_iota(jnp.int32, (tail_rows, token_count), 0)
            found = jnp.zeros((tail_rows, token_count), jnp.float32)
            for expert in range(experts):
                begin = expert * tail
                wanted = (order - begin + main).astype(jnp.float32)
                hit = ranks[expert : expert + 1, :] == wanted
                inside = jnp.logical_and(order >= begin, order < begin + tail)
                found = jnp.where(jnp.logical_and(hit, inside), 1.0, found)
            parts.append(found)
        pick = jnp.concatenate(parts, axis=0).astype(jnp.bfloat16)
        rows_in = jnp.dot(pick, block, preferred_element_type=jnp.float32)
        arrived[slot] = rows_in.astype(jnp.bfloat16)

    def tail_select(value_of, width):
        order = lax.broadcasted_iota(jnp.int32, (ep_slots, tail_rows, width), 1)
        order = order.reshape(ep_slots * tail_rows, width)
        total = value_of(0)
        for expert in range(1, experts):
            total = jnp.where(order >= expert * tail, value_of(expert), total)
        return total

    def gather(slot):
        if staged is None:
            gather_block(slot, tokens[slot])
        else:
            fetch = pltpu.make_async_copy(tokens.at[slot], staged, stage_sem.at[0])
            fetch.start()
            fetch.wait()
            gather_block(slot, staged[...])

    def share_stage():
        loop(ep_count - 1, lambda turn: rank_copy(ep_at(turn), ep_at(turn)).wait_recv())
        gather_block(me, normed_ref[...])
        loop(chips - 1, share_blocks)

    def up_stage():
        def finish_block(index):
            slot = index * CORES + other
            block_copy(tokens.at[slot], slot).wait_recv()
            gather(slot)

        finish_block(chip)
        loop(chips - 1, lambda turn: finish_block(chip_at(turn)))
        for one in weights[2:4]:
            one.wait()
        depth = arrived.shape[2]
        if tail_rows:
            block = arrived[:, tail_at:, :].reshape(ep_slots * tail_rows, depth)
            both = tail_select(
                lambda e: jnp.dot(block, gate_up[e], preferred_element_type=jnp.float32),
                2 * LANES,
            )
            hidden_tail[tp_me] = silu_mul(both)
            loop(tp_count - 1, lambda way: hidden_copy(tp_me, experts, tp_at(way)).start())
        if main:

            def expert_step(expert):
                span = pl.ds(pl.multiple_of(expert * main, main), main)
                block = arrived[:, span, :].reshape(ep_slots * main, depth)
                both = jnp.dot(block, gate_up[expert], preferred_element_type=jnp.float32)
                hidden_main[tp_me, expert] = silu_mul(both)
                loop(tp_count - 1, lambda way: hidden_copy(tp_me, expert, tp_at(way)).start())

            loop(experts, expert_step)

    def down_stage():
        weights[4].wait()
        width = down.shape[2]

        def arrival(part):
            loop(tp_count - 1, lambda way: hidden_copy(tp_at(way), part, tp_me).wait_recv())

        if tail_rows:
            arrival(experts)
            block = jnp.concatenate([hidden_tail[piece] for piece in range(tp_slots)], axis=1)
            out = tail_select(
                lambda e: jnp.dot(block, down[e], preferred_element_type=jnp.float32), width
            )
            out = out.astype(jnp.bfloat16).reshape(ep_slots, tail_rows, width)
            results[:, tail_at:, :] = out
        if main:

            def expert_step(expert):
                arrival(expert)
                span = pl.ds(pl.multiple_of(expert * main, main), main)
                pieces = [hidden_main[piece, expert] for piece in range(tp_slots)]
                block = jnp.concatenate(pieces, axis=1)
                out = jnp.dot(block, down[expert], preferred_element_type=jnp.float32)
                results[:, span, :] = out.astype(jnp.bfloat16).reshape(ep_slots, main, width)

            loop(experts, expert_step)
        loop(ep_count - 1, lambda turn: result_copy(ep_at(turn), me).start())
        returned[me] = results[me]

    def ratio(sums, head):
        whole = sums[head]
        return whole / pltpu.roll(whole, HEAD, 1)

    def pair_out(sums, pair):
        joined = ratio(sums, pair * group)
        if group == 1:
            joined = jnp.where(lane < HEAD, joined, 0.0)
        else:
            joined = jnp.where(lane < HEAD, joined, ratio(sums, pair * group + 1))
        return joined.astype(jnp.bfloat16)

    def send_guest(pair):
        guest_out[pair] = pair_out(guest_acc, pair)
        stats = jnp.zeros((rows, LANES), jnp.float32)
        for member in range(group):
            whole = guest_acc[pair * group + member]
            total = jnp.where(lane // HEAD == member, pltpu.roll(whole, HEAD, 1), whole)
            value = guest_max[pair * group + member] + jnp.log(total)
            stats = jnp.where(lane == member, value, stats)
        guest_lse[pair] = stats.T[:8, :]
        guest_result(pair).start()
        guest_stats(pair).start()

    def merge_guest(pair):
        guest_result(pair).wait_recv()
        guest_stats(pair).wait_recv()
        stats = jnp.concatenate([lse_in[pair]] * (LANES // 8), axis=0).T
        outer = guest_in[pair].astype(jnp.float32)
        for member in range(group):
            head = pair * group + member
            value = jnp.broadcast_to(stats[:, member : member + 1], (rows, LANES))
            new_max = jnp.maximum(row_max[head], value)
            part = jnp.where(lane // HEAD == member, outer, 1.0)
            acc[head] = acc[head] * jnp.exp(row_max[head] - new_max) + part * jnp.exp(
                value - new_max
            )

    def finish_pair(pair):
        if guests:

            @pl.when(chip == last)
            def _():
                merge_guest(pair)

        if wide_heads:
            heads_all[:, lanes_at(tp_me * pairs + pair, LANES)] = pair_out(acc, pair)
        else:
            heads_all[tp_me] = pair_out(acc, pair)
        loop(tp_count - 1, lambda way: heads_copy(tp_me, pair, tp_at(way)).start())

    reach = 1 if guests else chips
    deepest = jnp.where(chip == last, jnp.minimum(chip, reach), chip)
    step_count = deepest * CORES + core
    steps = max(CORES * (limit if guests else last) + 1, CORES + 1)
    delay = 3 if guests else 1
    total = pairs * (steps + 1)

    def remote_step(pair, step):
        turn = step - core + CORES
        own_core = turn % CORES == 0
        back = turn // CORES
        slot = (chip - back) * CORES + jnp.where(own_core, core, other)
        side_copy(slot, pair).wait_recv()

        @pl.when(jnp.logical_and(own_core, chip < (limit if guests else last)))
        def _():
            up_copy(slot, pair).start()

        @pl.when(own_core)
        def _():
            side_copy(slot, pair).start()

        attend(pair, slot, q_own, acc, row_max, False)
        if guests:

            @pl.when(chip == host)
            def _():
                attend(pair, slot, q_guest, guest_acc, guest_max, False)

    def start_guest(pair):
        guest_query(pair).wait_recv()
        for member in range(group):
            head = pair * group + member
            guest_acc[head] = jnp.zeros((rows, LANES), jnp.float32)
            guest_max[head] = jnp.full((rows, LANES), neg_fill, jnp.float32)

        def own_chip(turn):
            pl.when(turn > 0)(lambda: side_copy(me + 1, pair).wait_recv())
            attend(pair, me + turn, q_guest, guest_acc, guest_max, False)

        loop(CORES - core, own_chip)

    hooks = (
        (1, shared_stage),
        (1, spread_stage),
        (pairs, token_stage),
        (pairs + 1, share_stage),
        (pairs + 2, up_stage),
        (total, down_stage),
    )

    def one_turn(index):
        for at, stage in hooks:
            pl.when(index == at)(stage)

        @pl.when(index < pairs)
        def _():
            attend(index, me, q_own, acc, row_max, True)

        @pl.when(jnp.logical_and(index >= pairs, index < total))
        def _():
            pair = (index - pairs) // steps
            step = (index - pairs) % steps

            if guests:

                @pl.when(jnp.logical_and(chip == host, step == 0))
                def _():
                    start_guest(pair)

            @pl.when(step < step_count)
            def _():
                remote_step(pair, step)

            if guests:

                @pl.when(jnp.logical_and(chip == host, step == steps - 1))
                def _():
                    send_guest(pair)

        late = index - pairs - jnp.where(chip == last, delay, 0)

        @pl.when(jnp.logical_and(late >= 0, late < pairs * steps))
        def _():
            @pl.when(late % steps == steps - 1)
            def _():
                finish_pair(late // steps)

    loop(total + delay, one_turn)

    for pair in range(pairs):

        def finish_kv(back):
            slot = (chip - back) * CORES + core

            @pl.when(
                jnp.logical_or(
                    chip < (limit if guests else last), jnp.logical_and(back == 0, chip < last)
                )
            )
            def _():
                up_copy(slot, pair).wait_send()

            @pl.when(back > 0)
            def _():
                side_copy(slot, pair).wait_send()

        loop(deepest + 1, finish_kv)

        @pl.when(jnp.logical_or(core == 0, paired))
        def _():
            side_copy(me, pair).wait_send()

        if guests:

            @pl.when(chip == last)
            def _():
                guest_query(pair).wait_send()

            @pl.when(chip == host)
            def _():
                guest_result(pair).wait_send()
                guest_stats(pair).wait_send()

    def finish_tokens(turn):
        target = chip_at(turn)
        slot = target * CORES + core
        pl.when(jnp.logical_and(target < chip, higher))(lambda: hop_copy(slot, 0).wait_send())
        pl.when(jnp.logical_and(target > chip, lower))(lambda: hop_copy(slot, 1).wait_send())
        if relay:
            for way, peer in enumerate((x_peer, y_peer)):
                near_copy(slot, tp_me, way).wait_send()
                half_copy(slot, peer, way).wait_send()
        else:
            loop(tp_count - 1, lambda way: plane_copy(slot, tp_me, tp_at(way)).wait_send())
        block_copy(tokens.at[slot], slot).wait_send()

    loop(chips - 1, finish_tokens)
    pl.when(higher)(lambda: own_hop(0).wait_send())
    pl.when(lower)(lambda: own_hop(1).wait_send())
    block_copy(normed_ref, me).wait_send()

    def finish_peers(turn):
        rank_copy(ep_at(turn), me).wait_send()
        result_copy(ep_at(turn), me).wait_send()
        result_copy(ep_at(turn), ep_at(turn)).wait_recv()

    loop(ep_count - 1, finish_peers)

    def finish_plane(way):
        peer = tp_at(way)
        shared_copy(tp_me, peer).wait_send()
        shared_copy(peer, peer).wait_recv()
        for part in range(experts + 1):
            if tail_rows if part == experts else main:
                hidden_copy(tp_me, part, peer).wait_send()
        for pair in range(pairs):
            heads_copy(tp_me, pair, peer).wait_send()
            heads_copy(peer, pair, peer).wait_recv()

    loop(tp_count - 1, finish_plane)
    for one in weights[5:]:
        one.wait()
    shared_hidden = jnp.concatenate([shared_all[piece] for piece in range(tp_slots)], axis=1)
    back = returned[...].reshape(ep_slots * slot_rows, returned.shape[2])
    sums = jnp.dot(shared_hidden, shared_last[...], preferred_element_type=jnp.float32)
    for part in (spread_high, spread_low):
        sums = sums + jnp.dot(part[...], back, preferred_element_type=jnp.float32)
    moe_out[...] = sums.astype(jnp.bfloat16)
    if wide_heads:
        mixed = heads_all[...]
    else:
        mixed = jnp.concatenate([heads_all[piece] for piece in range(tp_slots)], axis=1)
    mixed = jnp.dot(mixed, mix_weight[...], preferred_element_type=jnp.float32)
    mixer_out[...] = mixed.astype(jnp.bfloat16)


def slot_layout(capacity, experts):
    main = capacity // ROW_TILE * ROW_TILE
    tail = capacity - main
    tail_rows = -(-tail * experts // ROW_TILE) * ROW_TILE
    return main, tail, experts * main + tail_rows


def padded(a, axis, to):
    if a.shape[axis] == to:
        return a
    spare = [(0, 0)] * a.ndim
    spare[axis] = (0, to - a.shape[axis])
    return jnp.pad(a, spare)


def fused_block(
    query_rows,
    key_rows,
    value_rows,
    cum_gate,
    routes,
    route_weight,
    moe_gain,
    moe_input,
    expert_gate,
    expert_up,
    expert_down,
    shared_gate,
    shared_up,
    shared_down,
    out_weight,
):
    rows, width = query_rows.shape
    heads = width // HEAD
    pairs = (heads + 1) // 2
    ep_count = lax.axis_size("ep")
    tp_count = lax.axis_size("tp")
    chips = ep_count // CORES
    lanes = pairs * LANES
    tile = rows // 2 if rows % (2 * LANES) == 0 else rows
    query_rows, key_rows, value_rows = (
        padded(a, 1, lanes) for a in (query_rows, key_rows, value_rows)
    )
    experts, depth, span = expert_gate.shape
    columns = expert_down.shape[2]
    token_count = moe_input.shape[0]
    capacity = 2 * token_count * routes.shape[1] // (experts * ep_count)
    main, tail, slot_rows = slot_layout(capacity, experts)
    if span < LANES:
        expert_gate, expert_up = padded(expert_gate, 2, LANES), padded(expert_up, 2, LANES)
        shared_gate, shared_up = padded(shared_gate, 1, LANES), padded(shared_up, 1, LANES)
        expert_down = padded(expert_down.reshape(experts, tp_count, span, columns), 2, LANES)
        expert_down = expert_down.reshape(experts, tp_count * LANES, columns)
        shared_down = padded(shared_down.reshape(tp_count, span, columns), 1, LANES)
        shared_down = shared_down.reshape(tp_count * LANES, columns)
    inside = ep_count * token_count * depth * 2 <= 8 * 1024 * 1024
    bf16, f32 = jnp.bfloat16, jnp.float32
    vmem = pl.BlockSpec(memory_space=pltpu.VMEM)
    anywhere = pl.BlockSpec(memory_space=pl.ANY)
    if width % LANES:
        out_weight = padded(out_weight.reshape(tp_count, width, columns), 1, LANES)
        out_weight = out_weight.reshape(tp_count * LANES, columns)
    heads_shape = (rows, tp_count * width) if width % LANES == 0 else (tp_count, rows, LANES)
    outs = [
        jax.ShapeDtypeStruct((rows, columns), bf16),
        jax.ShapeDtypeStruct((token_count, columns), bf16),
    ]
    out_specs = [vmem] * 2
    token_shape = (ep_count, token_count, depth)
    scratch = []
    if inside:
        scratch.append(pltpu.VMEM(token_shape, bf16))
    else:
        outs.append(jax.ShapeDtypeStruct(token_shape, bf16))
        out_specs.append(anywhere)
    dma = pltpu.SemaphoreType.DMA
    scratch += [
        pltpu.VMEM((token_count, depth), bf16),
        pltpu.VMEM((token_count, depth), bf16),
        pltpu.VMEM((ep_count, experts, token_count), f32),
        pltpu.VMEM(heads_shape, bf16),
        pltpu.VMEM((ep_count, slot_rows, columns), bf16),
        pltpu.VMEM((tp_count, token_count, LANES), bf16),
        pltpu.VMEM((token_count, ep_count * slot_rows), bf16),
        pltpu.VMEM((token_count, ep_count * slot_rows), bf16),
        pltpu.VMEM(out_weight.shape, bf16),
        pltpu.VMEM(shared_down.shape, bf16),
        pltpu.VMEM((rows, lanes), bf16),
        pltpu.VMEM((rows, lanes), bf16),
        pltpu.VMEM((ep_count, pairs, 2, rows, LANES), bf16),
        pltpu.VMEM((heads, rows, LANES), f32),
        pltpu.VMEM((heads, rows, LANES), f32),
        pltpu.VMEM((heads, rows, LANES), f32),
        pltpu.VMEM((heads, rows, LANES), f32),
        pltpu.VMEM((pairs, rows, LANES), bf16),
        pltpu.VMEM((pairs, rows, LANES), bf16),
        pltpu.VMEM((pairs, 8, rows), f32),
        pltpu.VMEM((pairs, 8, rows), f32),
        pltpu.VMEM((tile, rows), f32),
        pltpu.VMEM((tile, rows), f32),
        pltpu.VMEM((tile, LANES), f32),
        pltpu.VMEM((tile, LANES), f32),
        pltpu.VMEM((ep_count, experts, token_count), f32),
    ]
    if not inside:
        scratch.append(pltpu.VMEM((token_count, depth), bf16))
    scratch += [
        pltpu.VMEM((ep_count, slot_rows, depth), bf16),
        pltpu.VMEM((experts, depth, 2 * LANES), bf16),
        pltpu.VMEM(expert_down.shape, bf16),
        pltpu.VMEM((depth, 2 * LANES), bf16),
        pltpu.VMEM((tp_count, experts, ep_count * max(main, 1), LANES), bf16),
        pltpu.VMEM((tp_count, max(ep_count * (slot_rows - experts * main), 8), LANES), bf16),
        pltpu.VMEM((ep_count, slot_rows, columns), bf16),
        dma((9 + 2 * pairs,)),
        dma((ep_count, pairs)),
        dma((ep_count, pairs)),
        dma((ep_count, pairs)),
        dma((3, pairs)),
        dma((3, pairs)),
        dma((ep_count, 2)),
        dma((ep_count, tp_count)),
        dma((ep_count, tp_count)),
        dma((ep_count, 2)),
        dma((ep_count,)),
        dma((ep_count,)),
        dma((ep_count,)),
        dma((ep_count,)),
        dma((tp_count,)),
        dma((tp_count,)),
        dma((experts + 1, tp_count)),
        dma((experts + 1, tp_count)),
        dma((pairs, tp_count)),
        dma((pairs, tp_count)),
        dma((ep_count,)),
        dma((ep_count,)),
        dma((2,)),
    ]
    body = functools.partial(block_kernel, heads, main, tail)
    inputs = 15

    def kernel(*refs):
        refs = list(refs)
        if inside:
            refs.insert(inputs + 2 + 27, None)
        body(*refs)

    blocks = ep_count * rows * rows * heads
    return pl.pallas_call(
        kernel,
        out_shape=outs,
        in_specs=[anywhere] * 3 + [vmem] * 4 + [anywhere] * 8,
        out_specs=out_specs,
        scratch_shapes=scratch,
        compiler_params=pltpu.CompilerParams(
            collective_id=0, has_side_effects=True, vmem_limit_bytes=58 * 1024 * 1024
        ),
        cost_estimate=pl.CostEstimate(
            flops=blocks * 2 * 512, bytes_accessed=8 * 1024 * 1024, transcendentals=blocks
        ),
        name="fused_block",
    )(
        query_rows,
        key_rows,
        value_rows,
        cum_gate,
        routes.T,
        route_weight.T,
        moe_gain[None, :],
        moe_input,
        expert_gate,
        expert_up,
        expert_down,
        shared_gate,
        shared_up,
        shared_down,
        out_weight,
    )[:2]


def local(
    query_rows,
    key_rows,
    value_rows,
    cum_gate,
    out_weight,
    moe_input,
    moe_gain,
    routes,
    route_weight,
    expert_gate,
    expert_up,
    expert_down,
    shared_gate,
    shared_up,
    shared_down,
):
    mixer, moe = fused_block(
        query_rows,
        key_rows,
        value_rows,
        cum_gate,
        routes,
        route_weight,
        moe_gain,
        moe_input,
        expert_gate,
        expert_up,
        expert_down,
        shared_gate,
        shared_up,
        shared_down,
        out_weight,
    )
    return (mixer, moe)


def solution(mesh):
    placed = (
        P("ep", "tp"),
        P("ep", "tp"),
        P("ep", "tp"),
        P("tp", None),
        P(None, "tp"),
        P("ep", None),
        P(),
        P("ep", None),
        P("ep", None),
        P("ep", None, "tp"),
        P("ep", None, "tp"),
        P("ep", None, "tp"),
        P(None, "tp"),
        P(None, "tp"),
        P(None, "tp"),
    )
    return jax.shard_map(
        local, mesh=mesh, in_specs=placed, out_specs=(P("ep", "tp"), P("ep", "tp")), check_vma=False
    )
```
